32 devices in a mesh: sp: 8 (over z, x), tp: 4 (over y, core).
Axes of the slice: x: 2, y: 2, z: 4, core: 2. Of those that a mesh axis runs over, the one named last changes fastest.
Arguments:
- queries: bfloat16 [3072, 768], P('sp', 'tp'), may hold values from -8 to 8
- keys: bfloat16 [3072, 256], P('sp', 'tp'), may hold values from -8 to 8
- values: bfloat16 [3072, 256], P('sp', 'tp'), may hold values from -6 to 6
- sinks: float32 [12], P('tp'), may hold values from 1 to 6
- residual: bfloat16 [3072, 2048], P('sp'), may hold values from -6 to 6
- out_weight: bfloat16 [768, 2048], replicated, may hold values from -3 to 3
- norm_gain: float32 [2048], replicated, may hold values from 0.1 to 1.9
- shared_gate: bfloat16 [2048, 512], P(None, 'tp'), may hold values from -0.125 to 0.125
- shared_up: bfloat16 [2048, 512], P(None, 'tp'), may hold values from -0.125 to 0.125
- shared_down: bfloat16 [512, 2048], P('tp'), may hold values from -0.25 to 0.25
- expert_ids: int32 [3072, 2], P('sp'), may hold values from 0 to 15, all different within a row; in each aligned block of 96 rows (0 to 95, 96 to 191, ...) at most 24 rows name the same one
- route_weights: float32 [3072, 2], P(('sp', 'tp')), may hold values from 0.2 to 2
- expert_gate: bfloat16 [16, 2048, 1024], P('sp', None, 'tp'), may hold values from -0.125 to 0.125
- expert_up: bfloat16 [16, 2048, 1024], P('sp', None, 'tp'), may hold values from -0.125 to 0.125
- expert_down: bfloat16 [16, 1024, 2048], P('sp', 'tp'), may hold values from -0.1875 to 0.1875
Outputs:
- layer_out: bfloat16 [3072, 2048], P(('sp', 'tp'))
The draws below stay inside these ranges and needn't reach their ends.
Inputs may be any that keep to these rules, and one draw needn't show every extreme that they name: `expert_ids`: each row names 2 different experts. In each aligned block of 96 rows no expert is named more than 24 times, a bound that some blocks reach.
All inputs are finite; a program needn't handle non-finite values.
Results may differ from the reference program's by a relative error of at most 0.018.
Values may be sent and summed in bfloat16 or wider, within the bound.
A program may use at most 128 MiB of HBM per device.

```python
import math
import jax
import jax.numpy as jnp
import numpy as np
from jax import lax

D = 2048
HEADS = 12
KV_HEADS = 4
HEAD_DIM = 64
WINDOW = 128
GRID_W = 64
EXP_HID = 1024
SHARED_HID = 512
TOPK = 2
TOKENS = 3072
OWN = 96
EXPERTS = 16
CAP = 24
N_TP = 4


def drawn_pair(key):
    seeded = jax.random.fold_in(key, 7)
    query_seed, key_seed = jax.random.split(seeded, 2)
    queries = jnp.clip(jax.random.normal(query_seed, (TOKENS, HEADS, HEAD_DIM), jnp.float32), -6.0, 6.0)
    keys = jnp.clip(jax.random.normal(key_seed, (TOKENS, KV_HEADS, HEAD_DIM), jnp.float32), -6.0, 6.0)
    return (queries.reshape(TOKENS, HEADS * HEAD_DIM), keys.reshape(TOKENS, KV_HEADS * HEAD_DIM))


def draw_queries(key, part):
    return drawn_pair(key)[0].astype(jnp.bfloat16)


def draw_keys(key, part):
    return drawn_pair(key)[1].astype(jnp.bfloat16)


def shard_levels(own_key, dims, shards, low, largest):
    def one(position, shards_of):
        draws = jax.random.uniform(jax.random.fold_in(jax.random.fold_in(own_key, 6), position), (shards_of,), jnp.float32, low / len(shards), largest / len(shards))
        return jnp.repeat(jnp.exp(draws), dims[position] // shards_of).reshape((-1,) + (1,) * (len(dims) - position - 1))

    loudness = one(*shards[0])
    for cut in shards[1:]:
        loudness = loudness * one(*cut)
    return loudness


def assign_block(rng, own, number, rows, amount, top, bound, slope):
    sequence = jax.random.permutation(rng, amount)
    packed, usual = portions_of(amount, rows * top, bound, slope, True), portions_of(amount, rows * top, bound, slope, False)
    places = jnp.arange(amount)

    def named(tallies, turn):
        used = int((tallies > 0).sum())
        fixed = max(1, used // 4)
        moved = fixed + (places - fixed + turn * (used - fixed)) % max(1, amount - fixed)
        return jnp.zeros((amount,), jnp.int32).at[sequence[jnp.where(places < fixed, places, moved)]].set(jnp.asarray(tallies, jnp.int32))

    tallies = jnp.where(number % 4 == 0, named(packed, number // 4), named(usual, number - number // 4 - 1))
    mixed = jax.random.permutation(jax.random.fold_in(own, 3), amount)
    source_of, receiver = mixed[0:amount // 2 * 2:2], mixed[1:amount // 2 * 2:2]
    room = jnp.minimum(tallies[source_of] - 1, bound - tallies[receiver]) // 2
    room = jnp.where((source_of == sequence[0]) | (receiver == sequence[0]) | (tallies[receiver] == 0), 0, jnp.maximum(room, 0))
    moved = jax.random.randint(jax.random.fold_in(own, 4), (amount // 2,), 0, 1 << 20) % (room + 1)
    tallies = tallies.at[source_of].add(-moved).at[receiver].add(moved)
    items = jnp.searchsorted(jnp.cumsum(tallies), jnp.arange(rows * top), side="right").astype(jnp.int32)
    listing = items.reshape(top, rows).T
    listing = listing[jax.random.permutation(jax.random.fold_in(own, 1), rows)]
    turn = jax.random.randint(jax.random.fold_in(own, 2), (rows, 1), 0, top)
    return jnp.take_along_axis(listing, (jnp.arange(top)[None, :] + turn) % top, axis=1)


def portions_of(amount, total, most, slope, full):
    portions = [(1 << 20) // math.isqrt(rank ** slope) + 1 for rank in range(1, amount + 1)]
    largest = most if full else min(most, max(-(-total // amount), total * portions[0] // sum(portions)))
    least = 1 if total - largest >= amount - 1 else 0
    counts, surplus = [largest] + [least] * (amount - 1), total - largest - least * (amount - 1)
    while surplus > 0:
        free = [i for i in range(1, amount) if counts[i] < largest] or [i for i in range(1, amount) if counts[i] < most]
        pool, budget = sum([portions[i] for i in free]), surplus
        for i in free:
            more = min(most - counts[i], max(1, budget * portions[i] // pool), surplus)
            counts[i] = counts[i] + more
            surplus = surplus - more
    return np.array(counts)


def centred(rng, shape, width, limit, cuts=(), kind=jnp.bfloat16):
    gain = shard_levels(rng, shape, cuts, -0.22, 0.18) if cuts else 1.0
    values = jax.random.normal(rng, shape, jnp.float32) * width * gain
    return jnp.minimum(jnp.maximum(values, -limit), limit).astype(kind)


def setup_inputs(seed: int = 0) -> dict:
    arg_keys = jax.random.split(jax.random.key(seed), 16)
    queries = draw_queries(jax.random.fold_in(arg_keys[15], 71), 0)
    keys = draw_keys(jax.random.fold_in(arg_keys[15], 71), 0)
    values = centred(arg_keys[2], (TOKENS, KV_HEADS * HEAD_DIM), 1.0, 6.0, ((0, 8), (1, 4)))
    sinks = jnp.clip(1.0 + 5.0 * jax.random.uniform(arg_keys[3], (HEADS,), jnp.float32) ** shard_levels(arg_keys[3], (HEADS,), ((0, 4),), -0.2, 0.2), 1.0, 6.0)
    residual = centred(arg_keys[4], (TOKENS, D), 1.0, 6.0, ((0, 8),))
    out_weight = centred(arg_keys[5], (HEADS * HEAD_DIM, D), 0.5, 3.0)
    norm_gain = jnp.clip(1.0 + 0.18 * jax.random.normal(arg_keys[6], (D,), jnp.float32), 0.1, 1.9)
    shared_gate = centred(arg_keys[7], (D, SHARED_HID), D ** -0.5, 0.125, ((1, 4),))
    shared_up = centred(arg_keys[8], (D, SHARED_HID), D ** -0.5, 0.125, ((1, 4),))
    shared_down = centred(arg_keys[9], (SHARED_HID, D), SHARED_HID ** -0.5, 0.25, ((0, 4),))
    expert_ids_keys = jax.random.split(jax.random.fold_in(arg_keys[10], 1), TOKENS // OWN)
    expert_ids_turns = jax.random.permutation(jax.random.fold_in(arg_keys[10], 3), TOKENS // OWN)
    expert_ids = jax.vmap(lambda own, number: assign_block(jax.random.fold_in(arg_keys[10], 2), own, number, OWN, EXPERTS, TOPK, CAP, 2))(expert_ids_keys, expert_ids_turns).reshape((TOKENS, TOPK))
    route_weights = jnp.clip(jnp.exp(math.log(2.0) - 2.3025851 * jax.random.uniform(arg_keys[11], (TOKENS, TOPK), jnp.float32) ** shard_levels(arg_keys[11], (TOKENS, TOPK), ((0, 32),), -0.2, 0.2)), 0.2, 2.0)
    expert_gate = centred(arg_keys[12], (EXPERTS, D, EXP_HID), D ** -0.5, 0.125, ((0, 8), (2, 4)))
    expert_up = centred(arg_keys[13], (EXPERTS, D, EXP_HID), D ** -0.5, 0.125, ((0, 8), (2, 4)))
    expert_down = centred(arg_keys[14], (EXPERTS, EXP_HID, D), EXP_HID ** -0.5, 0.1875, ((0, 8), (1, 4)))
    return {"queries": queries, "keys": keys, "values": values, "sinks": sinks, "residual": residual, "out_weight": out_weight, "norm_gain": norm_gain, "shared_gate": shared_gate, "shared_up": shared_up, "shared_down": shared_down, "expert_ids": expert_ids, "route_weights": route_weights, "expert_gate": expert_gate, "expert_up": expert_up, "expert_down": expert_down}


ROPE_BASE = 10000.0
NEG_LARGE = -1e+30
NORM_EPSILON = 1e-06

def rotary_turn(values, places, turn_sign):
    halfway = values.shape[-1] // 2
    quarter = halfway // 2
    spectrum = ROPE_BASE ** (-jnp.arange(0, halfway, 2, dtype=jnp.float32) / halfway)

    def rotate_by(segment, offsets_at):
        angles = turn_sign * offsets_at.astype(jnp.float32)[:, None] * spectrum[None, :]
        cosine = jnp.cos(angles)[:, None, :]
        sine_part = jnp.sin(angles)[:, None, :]
        former = segment[..., :quarter]
        latter = segment[..., quarter:]
        return jnp.concatenate([former * cosine - latter * sine_part, former * sine_part + latter * cosine], axis=-1)
    return jnp.concatenate([rotate_by(values[..., :halfway], places // GRID_W), rotate_by(values[..., halfway:], places % GRID_W)], axis=-1)

def attend(queries, keys, values, sinks):
    group_size = HEADS // KV_HEADS
    places = jnp.arange(TOKENS, dtype=jnp.int32)
    turned_queries = rotary_turn(queries.astype(jnp.float32).reshape(TOKENS, HEADS, HEAD_DIM), places, 1.0).astype(jnp.bfloat16)
    turned_keys = rotary_turn(keys.astype(jnp.float32).reshape(TOKENS, KV_HEADS, HEAD_DIM), places, 1.0).astype(jnp.bfloat16)
    margin = ((WINDOW, WINDOW), (0, 0), (0, 0))
    padded_keys = jnp.pad(turned_keys, margin)
    padded_values = jnp.pad(values.reshape(TOKENS, KV_HEADS, HEAD_DIM), margin)
    sink_logit = sinks.astype(jnp.float32).reshape(KV_HEADS, group_size)[:, :, None, None]

    def one_block(block_index):
        start_row = block_index * WINDOW
        block_queries = lax.dynamic_slice_in_dim(turned_queries, start_row, WINDOW, 0).reshape(WINDOW, KV_HEADS, group_size, HEAD_DIM)
        block_keys = lax.dynamic_slice_in_dim(padded_keys, start_row, 3 * WINDOW, 0)
        block_values = lax.dynamic_slice_in_dim(padded_values, start_row, 3 * WINDOW, 0)
        scores = jnp.einsum('qkgd,mkd->kgqm', block_queries.astype(jnp.float32), block_keys.astype(jnp.float32)) * HEAD_DIM ** (-0.5)
        query_at = start_row + jnp.arange(WINDOW, dtype=jnp.int32)
        key_at = start_row - WINDOW + jnp.arange(3 * WINDOW, dtype=jnp.int32)
        allowed = (jnp.abs(query_at[:, None] - key_at[None, :]) <= WINDOW) & (key_at >= 0)[None, :] & (key_at < TOKENS)[None, :]
        scores = jnp.where(allowed[None, None], scores, NEG_LARGE)
        highest = jnp.maximum(lax.optimization_barrier(jnp.max(scores, axis=-1, keepdims=True)), sink_logit)
        lifted = jnp.exp(scores - highest)
        denominator = lax.optimization_barrier(jnp.sum(lifted, axis=-1, keepdims=True)) + jnp.exp(sink_logit - highest)
        probabilities = (lifted / denominator).astype(jnp.bfloat16)
        result = jnp.einsum('kgqm,mkd->qkgd', probabilities.astype(jnp.float32), block_values.astype(jnp.float32))
        return result.astype(jnp.bfloat16).reshape(WINDOW, HEADS * HEAD_DIM)
    blocks = lax.map(one_block, jnp.arange(TOKENS // WINDOW, dtype=jnp.int32))
    return blocks.reshape(TOKENS, HEADS * HEAD_DIM)

def gated_hidden(gathered_rows, gate_weight, up_weight):
    gate_values = jnp.dot(gathered_rows, gate_weight, preferred_element_type=jnp.float32)
    up_values = jnp.dot(gathered_rows, up_weight, preferred_element_type=jnp.float32)
    return (jax.nn.silu(gate_values) * up_values).astype(jnp.bfloat16)

def block_sum(hidden, down_weight):
    piece_width = hidden.shape[1] // N_TP
    running_total = jnp.zeros((hidden.shape[0], down_weight.shape[1]), jnp.float32)
    for block_index in range(N_TP):
        block_term = jnp.dot(hidden[:, block_index * piece_width:(block_index + 1) * piece_width], down_weight[block_index * piece_width:(block_index + 1) * piece_width], preferred_element_type=jnp.float32)
        running_total = running_total + lax.optimization_barrier(block_term.astype(jnp.bfloat16)).astype(jnp.float32)
    return running_total

def reference(queries, keys, values, sinks, residual, out_weight, norm_gain, shared_gate, shared_up, shared_down, expert_ids, route_weights, expert_gate, expert_up, expert_down):
    attended = attend(queries, keys, values, sinks)
    projected = jnp.dot(attended, out_weight, preferred_element_type=jnp.float32)
    mixed_rows = (residual.astype(jnp.float32) + projected).astype(jnp.bfloat16)
    mixed_float = mixed_rows.astype(jnp.float32)
    scale_rows = lax.rsqrt(lax.optimization_barrier(jnp.mean(mixed_float * mixed_float, axis=-1, keepdims=True)) + NORM_EPSILON)
    normed = (mixed_float * scale_rows * norm_gain).astype(jnp.bfloat16)
    shared_out = block_sum(gated_hidden(normed, shared_gate, shared_up), shared_down)
    owners = TOKENS // OWN
    assigns = OWN * TOPK
    route_rows = expert_ids.reshape(owners, assigns)
    order_index = jnp.arange(assigns, dtype=jnp.int32)
    earlier = order_index[None, :] < order_index[:, None]
    rank_in_block = lax.optimization_barrier(jnp.sum(((route_rows[:, :, None] == route_rows[:, None, :]) & earlier[None]).astype(jnp.int32), axis=2))
    slot_index = route_rows * CAP + rank_in_block
    owner_index = jnp.arange(owners, dtype=jnp.int32)[:, None]
    token_of = owner_index * OWN + order_index[None, :] // TOPK
    slot_token = jnp.full((owners, EXPERTS * CAP), TOKENS, jnp.int32).at[owner_index, slot_index].set(token_of)
    slot_weight = jnp.zeros((owners, EXPERTS * CAP), jnp.float32).at[owner_index, slot_index].set(route_weights.astype(jnp.float32).reshape(owners, assigns))
    normed_pad = jnp.concatenate([normed, jnp.zeros((1, D), jnp.bfloat16)], axis=0)

    def one_expert(accumulated, expert):
        tokens_here = lax.dynamic_slice_in_dim(slot_token, expert * CAP, CAP, 1).reshape(-1)
        weights_here = lax.dynamic_slice_in_dim(slot_weight, expert * CAP, CAP, 1).reshape(-1)
        gathered_rows = normed_pad[tokens_here]
        hidden = gated_hidden(gathered_rows, expert_gate[expert], expert_up[expert])
        outcome = block_sum(hidden, expert_down[expert]).astype(jnp.bfloat16)
        accumulated = accumulated.at[tokens_here].add(weights_here[:, None] * outcome.astype(jnp.float32))
        return (accumulated, None)
    accumulated, unused = lax.scan(one_expert, jnp.zeros((TOKENS + 1, D), jnp.float32), jnp.arange(EXPERTS, dtype=jnp.int32))
    return (mixed_float + shared_out + accumulated[:TOKENS]).astype(jnp.bfloat16)
```

```python
import jax
import jax.numpy as jnp
import numpy as np
from jax import lax
from jax.experimental import pallas as pl
from jax.experimental.pallas import tpu as pltpu
from jax.sharding import PartitionSpec as P
import functools

MESH = pl.DeviceIdType.MESH
VMEM = pl.BlockSpec(memory_space=pltpu.VMEM)
VMEM_LIMIT = 60 * 1024 * 1024

HEAD_DIM = 64
WINDOW = 128
GRID_W = 64
TOPK = 2


ROPE_BASE = 10000.0
NEG_LARGE = -1e30
NORM_EPSILON = 1e-06


def extended(x, sides, width):
    for axis, dim in sides:
        size, length = (lax.axis_size(axis), x.shape[dim])
        up = [(i, (i + 1) % size) for i in range(size - 1)]
        down = [(j, i) for i, j in up]
        last = lax.slice_in_dim(x, length - width, length, axis=dim)
        initial = lax.slice_in_dim(x, 0, width, axis=dim)
        before = lax.ppermute(last, axis, up)
        after = lax.ppermute(initial, axis, down)
        x = jnp.concatenate([before, x, after], axis=dim)
    return x


def rotary_turn(values, places):
    heads = values.shape[1] // HEAD_DIM
    halfway = HEAD_DIM // 2
    quarter = halfway // 2
    column = np.arange(HEAD_DIM)
    swap = np.zeros((HEAD_DIM, HEAD_DIM), np.float32)
    for d in range(HEAD_DIM):
        if d % halfway < quarter:
            swap[d + quarter, d] = -1.0
        else:
            swap[d - quarter, d] = 1.0
    swap = jnp.asarray(np.kron(np.eye(heads, dtype=np.float32), swap), jnp.bfloat16)
    spectrum = ROPE_BASE ** (-jnp.arange(0, halfway, 2, dtype=jnp.float32) / halfway)
    spectrum = jnp.tile(spectrum, values.shape[1] // quarter)
    first_half = jnp.asarray(np.tile(column < halfway, heads))
    offsets = jnp.where(
        first_half[None, :], (places // GRID_W)[:, None], (places % GRID_W)[:, None]
    )
    angles = offsets.astype(jnp.float32) * spectrum[None, :]
    swapped = jnp.dot(values, swap, preferred_element_type=jnp.float32)
    return (values.astype(jnp.float32) * jnp.cos(angles) + swapped * jnp.sin(angles)).astype(
        jnp.bfloat16
    )


def attend_kernel(key_heads, total_rows, first_ref, sink_ref, q_ref, kv_ref, out_ref):
    first = first_ref[0]
    heads = q_ref.shape[1] // HEAD_DIM
    group = heads // key_heads
    shape = (WINDOW, 3 * WINDOW)
    row = lax.broadcasted_iota(jnp.int32, shape, 0)
    column = lax.broadcasted_iota(jnp.int32, shape, 1) - WINDOW
    near = jnp.abs(row - column) <= WINDOW
    for block in range(q_ref.shape[0] // WINDOW):
        start = block * WINDOW
        key_at = column + (first + start)
        allowed = near & (key_at >= 0) & (key_at < total_rows)
        for kh in range(key_heads):
            span = slice(start, start + 3 * WINDOW)
            key = kv_ref[span, kh * HEAD_DIM : (kh + 1) * HEAD_DIM]
            value = kv_ref[span, (key_heads + kh) * HEAD_DIM : (key_heads + kh + 1) * HEAD_DIM]
            for h in range(kh * group, (kh + 1) * group):
                query = q_ref[start : start + WINDOW, h * HEAD_DIM : (h + 1) * HEAD_DIM]
                scores = lax.dot_general(
                    query, key, (((1,), (1,)), ((), ())), preferred_element_type=jnp.float32
                ) * HEAD_DIM ** (-0.5)
                scores = jnp.where(allowed, scores, NEG_LARGE)
                sink = sink_ref[h]
                highest = jnp.maximum(jnp.max(scores, axis=1, keepdims=True), sink)
                lifted = jnp.exp(scores - highest)
                below = jnp.sum(lifted, axis=1, keepdims=True) + jnp.exp(sink - highest)
                chances = (lifted / below).astype(jnp.bfloat16)
                result = jnp.dot(chances, value, preferred_element_type=jnp.float32)
                out_ref[start : start + WINDOW, h * HEAD_DIM : (h + 1) * HEAD_DIM] = result.astype(
                    jnp.bfloat16
                )


def attend(first, sinks, turned, widened, key_heads, total_rows):
    smem = pl.BlockSpec(memory_space=pltpu.SMEM)
    return pl.pallas_call(
        functools.partial(attend_kernel, key_heads, total_rows),
        out_shape=jax.ShapeDtypeStruct(turned.shape, jnp.bfloat16),
        in_specs=[smem, smem, VMEM, VMEM],
        out_specs=VMEM,
        name="attend",
    )(first.reshape(1), sinks, turned, widened)


def places_of(token_split, width_split):
    sp_at = lax.axis_index("sp")
    tp_at = lax.axis_index("tp")
    pair = tp_at + 1 - 2 * (tp_at % 2)
    cross = (tp_at + width_split // 2) % width_split
    return sp_at, tp_at, pair, cross


def flipped(a, b, size):
    total, bit = 0, 1
    while bit < size:
        total = total + (lax.rem(lax.div(a, bit) + lax.div(b, bit), 2)) * bit
        bit *= 2
    return total


def dot32(a, b):
    return jnp.dot(a, b, preferred_element_type=jnp.float32)


def experts_kernel(
    token_split,
    width_split,
    capacity,
    ids_ref,
    weights_ref,
    mixed_ref,
    normed_ref,
    shared_gate_ref,
    shared_up_ref,
    shared_down_ref,
    gate_hbm,
    up_hbm,
    down_hbm,
    out_ref,
    gate_ref,
    up_ref,
    down_ref,
    hidden_ref,
    weigh_ref,
    outgoing,
    arrived,
    from_pair,
    to_cross,
    from_cross,
    back,
    shared_part,
    shared_pair,
    shared_cross,
    shared_got,
    load_sem,
    send,
    recv,
    shared_send,
    shared_recv,
):
    steps, _, rows, width = arrived.shape
    experts = gate_ref.shape[0]
    hid = gate_ref.shape[2]
    own = out_ref.shape[0]
    block_rows = normed_ref.shape[0]
    sp_at, tp_at, pair, cross = places_of(token_split, width_split)
    pair_cross = (pair + width_split // 2) % width_split

    loads = [
        pltpu.make_async_copy(source, target, load_sem.at[n])
        for n, (source, target) in enumerate(
            ((gate_hbm, gate_ref), (up_hbm, up_ref), (down_hbm, down_ref))
        )
    ]
    for load in loads:
        load.start()

    barrier = pltpu.get_barrier_semaphore()

    @pl.loop(1, token_split)
    def _(i):
        pl.semaphore_signal(
            barrier,
            inc=1,
            device_id=(flipped(sp_at, i, token_split), tp_at),
            device_id_type=MESH,
        )

    for partner in (pair, cross):
        pl.semaphore_signal(barrier, inc=1, device_id=(sp_at, partner), device_id_type=MESH)

    square = (block_rows, block_rows)
    before = lax.broadcasted_iota(jnp.int32, square, 0)
    after = lax.broadcasted_iota(jnp.int32, square, 1)
    earlier = (before < after) & (before // own == after // own)
    same_place = before == after
    ids_row = [ids_ref[k : k + 1, :] for k in range(TOPK)]
    ids_column = [
        jnp.sum(jnp.where(same_place, row, 0), axis=1, keepdims=True) for row in ids_row
    ]
    spots = []
    for k in range(TOPK):
        found = jnp.zeros(square, jnp.int32)
        for other in range(TOPK):
            found = found + ((ids_column[other] == ids_row[k]) & earlier).astype(jnp.int32)
        rank = jnp.sum(found, axis=0, keepdims=True)
        home = ids_row[k] // experts
        spots.append(home * rows + (ids_row[k] - home * experts) * capacity + rank)

    def block_spots(b):
        return [spot[:, b * own : (b + 1) * own] for spot in spots]

    own_spots = block_spots(0)
    for b in range(1, width_split):
        own_spots = [jnp.where(tp_at == b, x, y) for x, y in zip(block_spots(b), own_spots)]

    slot_at = lax.broadcasted_iota(jnp.int32, (rows, own), 0)

    def chosen(where_to, at):
        first = at * rows
        return (
            jnp.where(
                (where_to[0] - first == slot_at) | (where_to[1] - first == slot_at), 1.0, 0.0
            )
        ).astype(jnp.bfloat16)

    def remote(stage, i, source, target, where):
        return pltpu.make_async_remote_copy(
            src_ref=source,
            dst_ref=target,
            send_sem=send.at[stage, i],
            recv_sem=recv.at[stage, i],
            device_id=where,
            device_id_type=MESH,
        )

    def partner_of(i):
        return flipped(sp_at, i, token_split)

    def along(i):
        there = partner_of(i)
        return remote(0, i, outgoing.at[there], arrived.at[i, tp_at], (there, tp_at))

    def passed(stage, i, block, partner):
        piece = arrived.at[i, block]
        return remote(stage, i, piece, piece, (sp_at, partner))

    def over(i):
        return passed(1, i, tp_at, cross)

    def beside(i):
        return passed(2, i, tp_at, pair)

    def third(i):
        return passed(3, i, cross, pair)

    def pair_back(side, i):
        block = pair_cross if side == 0 else pair
        return remote(4 + side, i, arrived.at[i, block], from_pair.at[side, i], (sp_at, pair))

    def cross_back(i):
        return remote(6, i, to_cross.at[i], from_cross.at[i], (sp_at, cross))

    def home_copy(i):
        there = partner_of(i)
        return remote(7, i, outgoing.at[there], back.at[sp_at], (there, tp_at))

    def copy_shared(stage, source, target, partner):
        return pltpu.make_async_remote_copy(
            src_ref=source,
            dst_ref=target,
            send_sem=shared_send.at[stage],
            recv_sem=shared_recv.at[stage],
            device_id=(sp_at, partner),
            device_id_type=MESH,
        )

    def shared_side(side):
        block = pair_cross if side == 0 else pair
        return copy_shared(side, shared_part.at[block], shared_pair.at[side], pair)

    shared_over = copy_shared(2, shared_cross, shared_got, cross)

    pl.semaphore_wait(barrier, token_split + 1)

    own_start = pl.multiple_of(tp_at * own, own)

    @pl.loop(1, token_split)
    def _(i):
        there = partner_of(i)
        outgoing[there] = dot32(
            chosen(own_spots, there), normed_ref[pl.ds(own_start, own), :]
        ).astype(outgoing.dtype)
        along(i).start()

    for b in range(width_split):
        arrived[0, b] = dot32(
            chosen(block_spots(b), sp_at), normed_ref[b * own : (b + 1) * own, :]
        ).astype(arrived.dtype)

    for load in loads:
        load.wait()

    row_expert = lax.broadcasted_iota(jnp.int32, (width_split * rows, hid), 0) % rows // capacity
    tile = min(width, 512)

    def silu_times(gate_values, up_values):
        return gate_values / (1.0 + jnp.exp(-gate_values)) * up_values

    def work(i):
        x = arrived[i].reshape(width_split * rows, width)
        for e in range(experts):
            mine = silu_times(dot32(x, gate_ref[e]), dot32(x, up_ref[e]))
            hidden_ref[:, e * hid : (e + 1) * hid] = jnp.where(row_expert == e, mine, 0.0).astype(
                hidden_ref.dtype
            )

        @pl.loop(0, width // tile)
        def _(n):
            at = pl.ds(pl.multiple_of(n * tile, tile), tile)
            result = dot32(hidden_ref[...], down_ref[:, at]).astype(arrived.dtype)
            arrived[i, :, :, at] = result.reshape(width_split, rows, tile)

    def total(*terms):
        value = terms[0].astype(jnp.float32)
        for term in terms[1:]:
            value = value + term.astype(jnp.float32)
        return value

    def forward(i):
        along(i).wait_recv()
        over(i).start()
        beside(i).start()

    def shared_work():
        for b in range(width_split):
            here = normed_ref[b * own : (b + 1) * own, :]
            hidden = silu_times(
                dot32(here, shared_gate_ref[...]), dot32(here, shared_up_ref[...])
            ).astype(jnp.bfloat16)
            shared_part[b] = dot32(hidden, shared_down_ref[...]).astype(shared_part.dtype)
        shared_side(0).start()
        shared_side(1).start()

    def weigh_work():
        square = (own, own)
        eye = lax.broadcasted_iota(jnp.int32, square, 0) == lax.broadcasted_iota(
            jnp.int32, square, 1
        )
        slot_of = lax.broadcasted_iota(jnp.int32, (own, token_split * rows), 1)
        weigh = jnp.zeros((own, token_split * rows), jnp.float32)
        for k in range(TOPK):
            spot = jnp.sum(jnp.where(eye, own_spots[k], 0), axis=1, keepdims=True)
            weight = jnp.sum(
                jnp.where(eye, weights_ref[k : k + 1, :], 0.0), axis=1, keepdims=True
            )
            weigh = jnp.where(slot_of == spot, weight, weigh)
        coarse = weigh.astype(jnp.bfloat16)
        weigh_ref[:own, :] = coarse
        weigh_ref[own:, :] = (weigh - coarse.astype(jnp.float32)).astype(jnp.bfloat16)

    shared_work()

    @pl.loop(0, token_split + 1)
    def _(s):
        @pl.when(s < token_split)
        def _():
            @pl.when(s >= 1)
            def _():
                beside(s).wait()
                third(s).wait()
                over(s).wait_send()

            work(s)
            pair_back(0, s).start()
            pair_back(1, s).start()
            pair_back(0, s).wait_recv()
            to_cross[s] = total(arrived[s, cross], from_pair[0, s]).astype(to_cross.dtype)
            cross_back(s).start()

        @pl.when(s == 0)
        def _():
            shared_side(0).wait_recv()
            shared_cross[...] = total(shared_part[cross], shared_pair[0]).astype(
                shared_cross.dtype
            )
            shared_over.start()
            weigh_work()
            forward(1)

        @pl.when(s + 2 < token_split)
        def _():
            forward(s + 2)

        @pl.when(s + 1 < token_split)
        def _():
            over(s + 1).wait_recv()
            third(s + 1).start()

        @pl.when(s >= 1)
        def _():
            i = s - 1
            pair_back(1, i).wait_recv()
            cross_back(i).wait_recv()
            summed = total(arrived[i, tp_at], from_pair[1, i], from_cross[i]).astype(back.dtype)

            @pl.when(i == 0)
            def _():
                back[sp_at] = summed

            @pl.when(i >= 1)
            def _():
                along(i).wait_send()
                outgoing[partner_of(i)] = summed
                home_copy(i).start()

    shared_side(1).wait_recv()
    shared_over.wait_recv()

    @pl.loop(1, token_split)
    def _(i):
        home_copy(i).wait_recv()

    for n in range(width // tile):
        at = slice(n * tile, (n + 1) * tile)
        routed = dot32(
            weigh_ref[...], back[:, :, at].reshape(token_split * rows, tile)
        )
        out_ref[:, at] = (
            total(
                mixed_ref[pl.ds(own_start, own), at],
                shared_part[tp_at, :, at],
                shared_pair[1, :, at],
                shared_got[:, at],
            )
            + routed[:own]
            + routed[own:]
        ).astype(out_ref.dtype)

    @pl.loop(0, token_split)
    def _(i):
        pair_back(0, i).wait_send()
        pair_back(1, i).wait_send()
        cross_back(i).wait_send()

    @pl.loop(1, token_split)
    def _(i):
        home_copy(i).wait_send()

    shared_side(0).wait_send()
    shared_side(1).wait_send()
    shared_over.wait_send()


def routed_experts(
    ids, weights, mixed, normed, shared_gate, shared_up, shared_down, gate, up, down, sizes
):
    token_split, width_split = sizes
    experts, width, hid = gate.shape
    own = weights.shape[1]
    capacity = max(2, 2 * own * TOPK // (experts * token_split))
    rows = -(-experts * capacity // 16) * 16
    kind = mixed.dtype
    chunk = (rows, width)
    anywhere = pl.BlockSpec(memory_space=pl.ANY)
    return pl.pallas_call(
        functools.partial(experts_kernel, token_split, width_split, capacity),
        out_shape=jax.ShapeDtypeStruct((own, width), kind),
        in_specs=[VMEM] * 7 + [anywhere] * 3,
        out_specs=VMEM,
        scratch_shapes=[
            pltpu.VMEM(gate.shape, kind),
            pltpu.VMEM(up.shape, kind),
            pltpu.VMEM((experts * hid, width), kind),
            pltpu.VMEM((width_split * rows, experts * hid), kind),
            pltpu.VMEM((2 * own, token_split * rows), kind),
            pltpu.VMEM((token_split,) + chunk, kind),
            pltpu.VMEM((token_split, width_split) + chunk, kind),
            pltpu.VMEM((2, token_split) + chunk, kind),
            pltpu.VMEM((token_split,) + chunk, kind),
            pltpu.VMEM((token_split,) + chunk, kind),
            pltpu.VMEM((token_split,) + chunk, kind),
            pltpu.VMEM((width_split, own, width), kind),
            pltpu.VMEM((2, own, width), kind),
            pltpu.VMEM((own, width), kind),
            pltpu.VMEM((own, width), kind),
            pltpu.SemaphoreType.DMA((3,)),
            pltpu.SemaphoreType.DMA((8, token_split)),
            pltpu.SemaphoreType.DMA((8, token_split)),
            pltpu.SemaphoreType.DMA((3,)),
            pltpu.SemaphoreType.DMA((3,)),
        ],
        compiler_params=pltpu.CompilerParams(
            collective_id=1, has_side_effects=True, vmem_limit_bytes=VMEM_LIMIT
        ),
        name="experts",
    )(
        ids,
        weights,
        mixed,
        normed,
        shared_gate,
        shared_up,
        shared_down,
        gate,
        up,
        down.reshape(experts * hid, width),
    )


def per_device(
    queries,
    keys,
    values,
    sinks,
    residual,
    out_weight,
    norm_gain,
    shared_gate,
    shared_up,
    shared_down,
    expert_ids,
    route_weights,
    expert_gate,
    expert_up,
    expert_down,
):
    block_rows = queries.shape[0]
    width_split = lax.axis_size("tp")
    token_split = lax.axis_size("sp")
    width_index = lax.axis_index("tp")
    key_heads = keys.shape[1] // HEAD_DIM
    heads_local = queries.shape[1] // HEAD_DIM
    first_row = lax.axis_index("sp") * block_rows
    total_rows = token_split * block_rows
    places = first_row + jnp.arange(block_rows, dtype=jnp.int32)
    turned = rotary_turn(jnp.concatenate([queries, keys], axis=1), places)
    query_width = heads_local * HEAD_DIM
    joined = jnp.concatenate([turned[:, query_width:], values], axis=1)
    widened = extended(joined, (("sp", 0),), WINDOW)
    attended = attend(
        first_row, sinks, turned[:, :query_width], widened, key_heads, total_rows
    )
    model_width = out_weight.shape[1]
    projected = jnp.dot(
        lax.all_gather(attended, "tp", axis=1, tiled=True),
        out_weight,
        preferred_element_type=jnp.float32,
    )
    mixed_rows = (residual.astype(jnp.float32) + projected).astype(jnp.bfloat16)
    mixed_float = mixed_rows.astype(jnp.float32)
    scale_rows = lax.rsqrt(
        jnp.mean(mixed_float * mixed_float, axis=-1, keepdims=True) + NORM_EPSILON
    )
    normed = (mixed_float * scale_rows * norm_gain).astype(jnp.bfloat16)
    return routed_experts(
        expert_ids.T,
        route_weights.T,
        mixed_rows,
        normed,
        shared_gate,
        shared_up,
        shared_down,
        expert_gate,
        expert_up,
        expert_down,
        (token_split, width_split),
    )


def solution(mesh):
    placed = (
        P("sp", "tp"),
        P("sp", "tp"),
        P("sp", "tp"),
        P("tp"),
        P("sp", None),
        P(),
        P(),
        P(None, "tp"),
        P(None, "tp"),
        P("tp", None),
        P("sp", None),
        P(("sp", "tp"), None),
        P("sp", None, "tp"),
        P("sp", None, "tp"),
        P("sp", "tp", None),
    )
    return jax.shard_map(
        per_device, mesh=mesh, in_specs=placed, out_specs=P(("sp", "tp"), None), check_vma=False
    )
```

```python
import jax
import jax.numpy as jnp
import numpy as np
from jax import lax
from jax.experimental import pallas as pl
from jax.experimental.pallas import tpu as pltpu
from jax.sharding import PartitionSpec as P
import functools

MESH = pl.DeviceIdType.MESH
VMEM = pl.BlockSpec(memory_space=pltpu.VMEM)
VMEM_LIMIT = 60 * 1024 * 1024

HEAD_DIM = 64
WINDOW = 128
GRID_W = 64
TOPK = 2


ROPE_BASE = 10000.0
NEG_LARGE = -1e30
NORM_EPSILON = 1e-06


def extended(x, sides, width):
    for axis, dim in sides:
        size, length = (lax.axis_size(axis), x.shape[dim])
        up = [(i, (i + 1) % size) for i in range(size - 1)]
        down = [(j, i) for i, j in up]
        last = lax.slice_in_dim(x, length - width, length, axis=dim)
        initial = lax.slice_in_dim(x, 0, width, axis=dim)
        before = lax.ppermute(last, axis, up)
        after = lax.ppermute(initial, axis, down)
        x = jnp.concatenate([before, x, after], axis=dim)
    return x


def rotary_turn(values, places):
    heads = values.shape[1] // HEAD_DIM
    halfway = HEAD_DIM // 2
    quarter = halfway // 2
    column = np.arange(HEAD_DIM)
    swap = np.zeros((HEAD_DIM, HEAD_DIM), np.float32)
    for d in range(HEAD_DIM):
        if d % halfway < quarter:
            swap[d + quarter, d] = -1.0
        else:
            swap[d - quarter, d] = 1.0
    swap = jnp.asarray(np.kron(np.eye(heads, dtype=np.float32), swap), jnp.bfloat16)
    spectrum = ROPE_BASE ** (-jnp.arange(0, halfway, 2, dtype=jnp.float32) / halfway)
    spectrum = jnp.tile(spectrum, values.shape[1] // quarter)
    first_half = jnp.asarray(np.tile(column < halfway, heads))
    offsets = jnp.where(
        first_half[None, :], (places // GRID_W)[:, None], (places % GRID_W)[:, None]
    )
    angles = offsets.astype(jnp.float32) * spectrum[None, :]
    swapped = jnp.dot(values, swap, preferred_element_type=jnp.float32)
    return (values.astype(jnp.float32) * jnp.cos(angles) + swapped * jnp.sin(angles)).astype(
        jnp.bfloat16
    )


def attend_kernel(key_heads, total_rows, first_ref, sink_ref, q_ref, kv_ref, out_ref):
    first = first_ref[0]
    heads = q_ref.shape[1] // HEAD_DIM
    group = heads // key_heads
    shape = (WINDOW, 3 * WINDOW)
    row = lax.broadcasted_iota(jnp.int32, shape, 0)
    column = lax.broadcasted_iota(jnp.int32, shape, 1) - WINDOW
    near = jnp.abs(row - column) <= WINDOW
    for block in range(q_ref.shape[0] // WINDOW):
        start = block * WINDOW
        key_at = column + (first + start)
        allowed = near & (key_at >= 0) & (key_at < total_rows)
        for kh in range(key_heads):
            span = slice(start, start + 3 * WINDOW)
            key = kv_ref[span, kh * HEAD_DIM : (kh + 1) * HEAD_DIM]
            value = kv_ref[span, (key_heads + kh) * HEAD_DIM : (key_heads + kh + 1) * HEAD_DIM]
            for h in range(kh * group, (kh + 1) * group):
                query = q_ref[start : start + WINDOW, h * HEAD_DIM : (h + 1) * HEAD_DIM]
                scores = lax.dot_general(
                    query, key, (((1,), (1,)), ((), ())), preferred_element_type=jnp.float32
                ) * HEAD_DIM ** (-0.5)
                scores = jnp.where(allowed, scores, NEG_LARGE)
                sink = sink_ref[h]
                highest = jnp.maximum(jnp.max(scores, axis=1, keepdims=True), sink)
                lifted = jnp.exp(scores - highest)
                below = jnp.sum(lifted, axis=1, keepdims=True) + jnp.exp(sink - highest)
                chances = (lifted / below).astype(jnp.bfloat16)
                result = jnp.dot(chances, value, preferred_element_type=jnp.float32)
                out_ref[start : start + WINDOW, h * HEAD_DIM : (h + 1) * HEAD_DIM] = result.astype(
                    jnp.bfloat16
                )


def attend(first, sinks, turned, widened, key_heads, total_rows):
    smem = pl.BlockSpec(memory_space=pltpu.SMEM)
    return pl.pallas_call(
        functools.partial(attend_kernel, key_heads, total_rows),
        out_shape=jax.ShapeDtypeStruct(turned.shape, jnp.bfloat16),
        in_specs=[smem, smem, VMEM, VMEM],
        out_specs=VMEM,
        name="attend",
    )(first.reshape(1), sinks, turned, widened)


def flipped(a, b, size):
    total, bit = 0, 1
    while bit < size:
        total = total + (lax.rem(lax.div(a, bit) + lax.div(b, bit), 2)) * bit
        bit *= 2
    return total


def dot32(a, b):
    return jnp.dot(a, b, preferred_element_type=jnp.float32)


def total(*terms):
    value = terms[0].astype(jnp.float32)
    for term in terms[1:]:
        value = value + term.astype(jnp.float32)
    return value


def silu_times(gate_values, up_values):
    return gate_values / (1.0 + jnp.exp(-gate_values)) * up_values


def experts_kernel(
    token_split,
    capacity,
    ids_ref,
    weights_ref,
    mixed_ref,
    normed_ref,
    shared_gate_hbm,
    shared_up_hbm,
    shared_down_hbm,
    gate_hbm,
    up_hbm,
    down_hbm,
    out_ref,
    shared_gate,
    shared_up,
    shared_down,
    gate,
    up,
    down,
    column_rows,
    hidden,
    weigh_ref,
    outgoing,
    outgoing_other,
    arrived,
    part,
    from_cross,
    back,
    shared_part,
    shared_got,
    load_sem,
    weight_send,
    weight_recv,
    send,
    recv,
    shared_sem,
):
    _, experts, rows, width = arrived.shape
    hid = gate.shape[3]
    shared_hid = shared_down_hbm.shape[0]
    own = out_ref.shape[0]
    block_rows = normed_ref.shape[0]
    halves = experts
    sp_at = lax.axis_index("sp")
    tp_at = lax.axis_index("tp")
    column = lax.rem(tp_at, 2)
    half = lax.div(tp_at, 2)
    other = 1 - half
    pair = 2 * half + 1 - column
    cross = 2 * other + column

    def weight_pairs(which):
        side = pl.ds(which * shared_hid, shared_hid)
        return (
            (shared_gate_hbm, shared_gate.at[:, side]),
            (shared_up_hbm, shared_up.at[:, side]),
            (shared_down_hbm, shared_down.at[side, :]),
            (gate_hbm, gate.at[which]),
            (up_hbm, up.at[which]),
            (down_hbm, down.at[:, pl.ds(which * hid, hid), :]),
        )

    loads = [
        pltpu.make_async_copy(source, target, load_sem.at[n])
        for n, (source, target) in enumerate(weight_pairs(0))
    ]
    shares = [
        pltpu.make_async_remote_copy(
            src_ref=source,
            dst_ref=target,
            send_sem=weight_send.at[n],
            recv_sem=weight_recv.at[n],
            device_id=(sp_at, pair),
            device_id_type=MESH,
        )
        for n, (source, target) in enumerate(weight_pairs(1))
    ]
    for load in loads:
        load.start()

    barrier = pltpu.get_barrier_semaphore()

    @pl.loop(1, token_split)
    def _(i):
        pl.semaphore_signal(
            barrier,
            inc=1,
            device_id=(flipped(sp_at, i, token_split), tp_at),
            device_id_type=MESH,
        )

    for partner in (pair, cross):
        pl.semaphore_signal(barrier, inc=1, device_id=(sp_at, partner), device_id_type=MESH)

    square = (block_rows, block_rows)
    before = lax.broadcasted_iota(jnp.int32, square, 0)
    after = lax.broadcasted_iota(jnp.int32, square, 1)
    earlier = (before < after) & (before // own == after // own)
    same_place = before == after
    ids_row = [ids_ref[k : k + 1, :] for k in range(TOPK)]
    ids_column = [
        jnp.sum(jnp.where(same_place, row, 0), axis=1, keepdims=True) for row in ids_row
    ]
    half_row = lax.broadcasted_iota(jnp.int32, (1, block_rows), 1) // (2 * own)
    codes, spots = [], []
    for k in range(TOPK):
        found = jnp.zeros(square, jnp.int32)
        for another in range(TOPK):
            found = found + ((ids_column[another] == ids_row[k]) & earlier).astype(jnp.int32)
        rank = jnp.sum(found, axis=0, keepdims=True)
        home = ids_row[k] // experts
        spots.append(home * rows + (ids_row[k] - home * experts) * capacity + rank)
        codes.append(ids_row[k] * rows + half_row * capacity + rank)

    def block_of(row, b):
        return row[:, b * own : (b + 1) * own]

    def column_block(row, b):
        return jnp.where(column == 0, block_of(row, 2 * b), block_of(row, 2 * b + 1))

    column_codes = [
        jnp.concatenate([column_block(code, b) for b in range(halves)], axis=1) for code in codes
    ]
    own_spots = [
        jnp.where(half == 0, column_block(spot, 0), column_block(spot, 1)) for spot in spots
    ]
    slot_at = lax.broadcasted_iota(jnp.int32, (rows, halves * own), 0)

    def chosen(at, expert):
        wanted = slot_at + (at * experts + expert) * rows
        return jnp.where(
            (column_codes[0] == wanted) | (column_codes[1] == wanted), 1.0, 0.0
        ).astype(jnp.bfloat16)

    for b in range(halves):
        start = pl.multiple_of((2 * b + column) * own, own)
        column_rows[b * own : (b + 1) * own, :] = normed_ref[pl.ds(start, own), :]

    def remote(stage, i, source, target, where):
        return pltpu.make_async_remote_copy(
            src_ref=source,
            dst_ref=target,
            send_sem=send.at[stage, i],
            recv_sem=recv.at[stage, i],
            device_id=where,
            device_id_type=MESH,
        )

    def partner_of(i):
        return flipped(sp_at, i, token_split)

    near = token_split // 2
    middle = lax.rem(lax.div(sp_at, near) + lax.div(sp_at, max(1, near // 2)), 2)

    def in_order(step):
        return flipped(step, middle * (near // 2) * lax.div(step, near), token_split)

    def along(i):
        there = partner_of(i)
        return remote(0, i, outgoing.at[there], arrived.at[i, half], (there, tp_at))

    def along_other(i):
        there = partner_of(i)
        return remote(1, i, outgoing_other.at[i], arrived.at[i, other], (there, tp_at))

    def over(i):
        piece = arrived.at[i, half]
        return remote(1, i, piece, piece, (sp_at, cross))

    def cross_back(i):
        return remote(2, i, part.at[i, other], from_cross.at[i], (sp_at, cross))

    def home_copy(i):
        there = partner_of(i)
        return remote(3, i, outgoing.at[there], back.at[sp_at], (there, tp_at))

    shared_over = pltpu.make_async_remote_copy(
        src_ref=shared_part.at[other],
        dst_ref=shared_got,
        send_sem=shared_sem.at[0],
        recv_sem=shared_sem.at[1],
        device_id=(sp_at, cross),
        device_id_type=MESH,
    )

    pl.semaphore_wait(barrier, token_split + 1)

    for share in shares:
        share.start()

    @pl.loop(1, token_split)
    def _(step):
        i = 1 + lax.rem(step - 1 + middle * (near - 1), token_split - 1)
        there = partner_of(i)
        outgoing[there] = dot32(chosen(there, half), column_rows[...]).astype(outgoing.dtype)
        along(i).start()

        @pl.when(i < near)
        def _():
            outgoing_other[i] = dot32(chosen(there, other), column_rows[...]).astype(
                outgoing_other.dtype
            )
            along_other(i).start()

    for e in range(experts):
        arrived[0, e] = dot32(chosen(sp_at, e), column_rows[...]).astype(arrived.dtype)

    tile = min(width, 512)

    def work(i):
        for e in range(experts):
            x = arrived[i, e]
            for p in range(2):
                hidden[e, :, p * hid : (p + 1) * hid] = silu_times(
                    dot32(x, gate[p, e]), dot32(x, up[p, e])
                ).astype(hidden.dtype)

        @pl.loop(0, width // tile)
        def _(n):
            at = pl.ds(pl.multiple_of(n * tile, tile), tile)
            results = [dot32(hidden[e], down[e, :, at]) for e in range(experts)]
            for b in range(halves):
                if capacity % 8 == 0 and rows == experts * capacity:
                    piece = jnp.concatenate(
                        [result[b * capacity : (b + 1) * capacity] for result in results], axis=0
                    )
                else:
                    piece = jnp.zeros((rows, tile), jnp.float32)
                    into = lax.broadcasted_iota(jnp.int32, (rows, rows), 0)
                    source = lax.broadcasted_iota(jnp.int32, (rows, rows), 1)
                    for e in range(experts):
                        rank = into - e * capacity
                        picked = (
                            (rank >= 0) & (rank < capacity) & (source == rank + b * capacity)
                        )
                        piece = piece + dot32(
                            jnp.where(picked, 1.0, 0.0).astype(jnp.bfloat16),
                            results[e].astype(jnp.bfloat16),
                        )
                part[i, b, :, at] = piece.astype(part.dtype)

    def forward(step):
        i = in_order(step)
        along(i).wait_recv()

        @pl.when(step >= near)
        def _():
            over(i).start()

    def weigh_work():
        square = (own, own)
        eye = lax.broadcasted_iota(jnp.int32, square, 0) == lax.broadcasted_iota(
            jnp.int32, square, 1
        )
        slot_of = lax.broadcasted_iota(jnp.int32, (own, token_split * rows), 1)
        weigh = jnp.zeros((own, token_split * rows), jnp.float32)
        for k in range(TOPK):
            spot = jnp.sum(jnp.where(eye, own_spots[k], 0), axis=1, keepdims=True)
            weight = jnp.sum(
                jnp.where(eye, weights_ref[k : k + 1, :], 0.0), axis=1, keepdims=True
            )
            weigh = jnp.where(slot_of == spot, weight, weigh)
        coarse = weigh.astype(jnp.bfloat16)
        weigh_ref[:own, :] = coarse
        weigh_ref[own:, :] = (weigh - coarse.astype(jnp.float32)).astype(jnp.bfloat16)

    for n in range(3):
        loads[n].wait()
        shares[n].wait()
    shared_hidden = silu_times(
        dot32(column_rows[...], shared_gate[...]), dot32(column_rows[...], shared_up[...])
    ).astype(jnp.bfloat16)
    for n in range(width // tile):
        at = slice(n * tile, (n + 1) * tile)
        shared_part[:, :, at] = (
            dot32(shared_hidden, shared_down[:, at])
            .astype(shared_part.dtype)
            .reshape(halves, own, tile)
        )
    shared_over.start()
    weigh_work()
    for n in range(3, 6):
        loads[n].wait()
        shares[n].wait()

    @pl.loop(0, token_split + 1)
    def _(step):
        @pl.when(step < token_split)
        def _():
            i = in_order(step)

            @pl.when(step >= 1)
            def _():
                over(i).wait_recv()

            work(i)
            cross_back(i).start()

        @pl.when(step == 0)
        def _():
            forward(1)

        @pl.when(step >= 1)
        def _():
            i = in_order(step - 1)
            cross_back(i).wait_recv()
            summed = total(part[i, half], from_cross[i]).astype(back.dtype)

            @pl.when(step == 1)
            def _():
                back[sp_at] = summed

            @pl.when(step >= 2)
            def _():
                along(i).wait_send()
                outgoing[partner_of(i)] = summed
                home_copy(i).start()

        @pl.when(step + 2 < token_split)
        def _():
            forward(step + 2)

    shared_over.wait_recv()

    @pl.loop(1, token_split)
    def _(i):
        home_copy(i).wait_recv()

    own_start = pl.multiple_of(tp_at * own, own)
    for n in range(width // tile):
        at = slice(n * tile, (n + 1) * tile)
        routed = dot32(weigh_ref[...], back[:, :, at].reshape(token_split * rows, tile))
        out_ref[:, at] = (
            total(
                mixed_ref[pl.ds(own_start, own), at], shared_part[half, :, at], shared_got[:, at]
            )
            + routed[:own]
            + routed[own:]
        ).astype(out_ref.dtype)

    @pl.loop(0, token_split)
    def _(i):
        cross_back(i).wait_send()

    @pl.loop(1, token_split)
    def _(i):
        over(i).wait_send()
        home_copy(i).wait_send()

    shared_over.wait_send()


def routed_experts(
    ids, weights, mixed, normed, shared_gate, shared_up, shared_down, gate, up, down, sizes
):
    token_split, width_split = sizes
    experts, width, hid = gate.shape
    if experts != 2 or width_split != 4:
        raise ValueError("unsupported split")
    own = weights.shape[1]
    capacity = max(2, 2 * own * TOPK // (experts * token_split))
    rows = -(-experts * capacity // 16) * 16
    shared_hid = shared_gate.shape[1]
    kind = mixed.dtype
    chunk = (rows, width)
    hbm = pl.BlockSpec(memory_space=pltpu.HBM)
    dma = pltpu.SemaphoreType.DMA
    return pl.pallas_call(
        functools.partial(experts_kernel, token_split, capacity),
        out_shape=jax.ShapeDtypeStruct((own, width), kind),
        in_specs=[VMEM] * 4 + [hbm] * 6,
        out_specs=VMEM,
        scratch_shapes=[
            pltpu.VMEM((width, 2 * shared_hid), kind),
            pltpu.VMEM((width, 2 * shared_hid), kind),
            pltpu.VMEM((2 * shared_hid, width), kind),
            pltpu.VMEM((2, experts, width, hid), kind),
            pltpu.VMEM((2, experts, width, hid), kind),
            pltpu.VMEM((experts, 2 * hid, width), kind),
            pltpu.VMEM((2 * own, width), kind),
            pltpu.VMEM((experts, rows, 2 * hid), kind),
            pltpu.VMEM((2 * own, token_split * rows), kind),
            pltpu.VMEM((token_split,) + chunk, kind),
            pltpu.VMEM((token_split // 2,) + chunk, kind),
            pltpu.VMEM((token_split, experts) + chunk, kind),
            pltpu.VMEM((token_split, 2) + chunk, kind),
            pltpu.VMEM((token_split,) + chunk, kind),
            pltpu.VMEM((token_split,) + chunk, kind),
            pltpu.VMEM((2, own, width), kind),
            pltpu.VMEM((own, width), kind),
            dma((6,)),
            dma((6,)),
            dma((6,)),
            dma((4, token_split)),
            dma((4, token_split)),
            dma((2,)),
        ],
        compiler_params=pltpu.CompilerParams(
            collective_id=1, has_side_effects=True, vmem_limit_bytes=VMEM_LIMIT
        ),
        name="experts",
    )(ids, weights, mixed, normed, shared_gate, shared_up, shared_down, gate, up, down)


def per_device(
    queries,
    keys,
    values,
    sinks,
    residual,
    out_weight,
    norm_gain,
    shared_gate,
    shared_up,
    shared_down,
    expert_ids,
    route_weights,
    expert_gate,
    expert_up,
    expert_down,
):
    block_rows = queries.shape[0]
    width_split = lax.axis_size("tp")
    token_split = lax.axis_size("sp")
    width_index = lax.axis_index("tp")
    key_heads = keys.shape[1] // HEAD_DIM
    heads_local = queries.shape[1] // HEAD_DIM
    first_row = lax.axis_index("sp") * block_rows
    total_rows = token_split * block_rows
    places = first_row + jnp.arange(block_rows, dtype=jnp.int32)
    turned = rotary_turn(jnp.concatenate([queries, keys], axis=1), places)
    query_width = heads_local * HEAD_DIM
    joined = jnp.concatenate([turned[:, query_width:], values], axis=1)
    widened = extended(joined, (("sp", 0),), WINDOW)
    attended = attend(
        first_row, sinks, turned[:, :query_width], widened, key_heads, total_rows
    )
    model_width = out_weight.shape[1]
    projected = jnp.dot(
        lax.all_gather(attended, "tp", axis=1, tiled=True),
        out_weight,
        preferred_element_type=jnp.float32,
    )
    mixed_rows = (residual.astype(jnp.float32) + projected).astype(jnp.bfloat16)
    mixed_float = mixed_rows.astype(jnp.float32)
    scale_rows = lax.rsqrt(
        jnp.mean(mixed_float * mixed_float, axis=-1, keepdims=True) + NORM_EPSILON
    )
    normed = (mixed_float * scale_rows * norm_gain).astype(jnp.bfloat16)
    return routed_experts(
        expert_ids.T,
        route_weights.T,
        mixed_rows,
        normed,
        shared_gate,
        shared_up,
        shared_down,
        expert_gate,
        expert_up,
        expert_down,
        (token_split, width_split),
    )


def solution(mesh):
    placed = (
        P("sp", "tp"),
        P("sp", "tp"),
        P("sp", "tp"),
        P("tp"),
        P("sp", None),
        P(),
        P(),
        P(None, "tp"),
        P(None, "tp"),
        P("tp", None),
        P("sp", None),
        P(("sp", "tp"), None),
        P("sp", None, "tp"),
        P("sp", None, "tp"),
        P("sp", "tp", None),
    )
    return jax.shard_map(
        per_device, mesh=mesh, in_specs=placed, out_specs=P(("sp", "tp"), None), check_vma=False
    )
```

```python
import jax
import jax.numpy as jnp
import numpy as np
from jax import lax
from jax.experimental import pallas as pl
from jax.experimental.pallas import tpu as pltpu
from jax.sharding import PartitionSpec as P
import functools

MESH = pl.DeviceIdType.MESH
VMEM = pl.BlockSpec(memory_space=pltpu.VMEM)
VMEM_LIMIT = 62 * 1024 * 1024

HEAD_DIM = 64
WINDOW = 128
GRID_W = 64
TOPK = 2


ROPE_BASE = 10000.0
NEG_LARGE = -1e30
NORM_EPSILON = 1e-06


def turn_tables(total_rows):
    halfway = HEAD_DIM // 2
    spectrum = np.float32(ROPE_BASE) ** (
        -np.arange(0, halfway, 2, dtype=np.float32) / np.float32(halfway)
    )
    places = np.arange(total_rows)
    tables = []
    for offsets in (places // GRID_W, places % GRID_W):
        angles = spectrum[:, None].astype(np.float32) * offsets.astype(np.float32)[None, :]
        tables += [np.cos(angles), np.sin(angles)]
    return np.stack(tables).astype(np.float32)


def flipped(a, b, size):
    total, bit = 0, 1
    while bit < size:
        total = total + (lax.rem(lax.div(a, bit) + lax.div(b, bit), 2)) * bit
        bit *= 2
    return total


def dot32(a, b):
    return jnp.dot(a, b, preferred_element_type=jnp.float32)


def total(*terms):
    value = terms[0].astype(jnp.float32)
    for term in terms[1:]:
        value = value + term.astype(jnp.float32)
    return value


def silu_times(gate_values, up_values):
    return gate_values / (1.0 + jnp.exp(-gate_values)) * up_values


def layer_kernel(
    token_split,
    capacity,
    sinks_ref,
    queries_ref,
    keys_ref,
    values_ref,
    gain_ref,
    ids_ref,
    weights_ref,
    tables_hbm,
    residual_hbm,
    out_weight_hbm,
    shared_gate_hbm,
    shared_up_hbm,
    shared_down_hbm,
    gate_hbm,
    up_hbm,
    down_hbm,
    out_ref,
    tables,
    residual,
    out_weight,
    turned,
    near_keys,
    near_values,
    attended,
    gathered,
    summed_rows,
    mixed,
    shared_gate,
    shared_up,
    shared_down,
    gate,
    up,
    down,
    column_rows,
    hidden,
    weigh_ref,
    outgoing,
    outgoing_other,
    arrived,
    part,
    from_cross,
    back,
    shared_part,
    shared_got,
    load_sem,
    weight_send,
    weight_recv,
    send,
    recv,
    shared_sem,
    first_sem,
    halo_send,
    halo_recv,
    gather_send,
    gather_recv,
):
    _, experts, rows, width = arrived.shape
    hid = gate.shape[3]
    shared_hid = shared_down_hbm.shape[0]
    own = out_ref.shape[0]
    block_rows = queries_ref.shape[1]
    halves = experts
    sp_at = lax.axis_index("sp")
    tp_at = lax.axis_index("tp")
    column = lax.rem(tp_at, 2)
    half = lax.div(tp_at, 2)
    other = 1 - half
    pair = 2 * half + 1 - column
    cross = 2 * other + column
    diagonal = 2 * other + 1 - column

    def weight_pairs(which):
        side = pl.ds(which * shared_hid, shared_hid)
        return (
            (shared_gate_hbm, shared_gate.at[:, side]),
            (shared_up_hbm, shared_up.at[:, side]),
            (shared_down_hbm, shared_down.at[side, :]),
            (gate_hbm, gate.at[which]),
            (up_hbm, up.at[which]),
            (down_hbm, down.at[:, pl.ds(which * hid, hid), :]),
        )

    loads = [
        pltpu.make_async_copy(source, target, load_sem.at[n])
        for n, (source, target) in enumerate(weight_pairs(0))
    ]
    shares = [
        pltpu.make_async_remote_copy(
            src_ref=source,
            dst_ref=target,
            send_sem=weight_send.at[n],
            recv_sem=weight_recv.at[n],
            device_id=(sp_at, pair),
            device_id_type=MESH,
        )
        for n, (source, target) in enumerate(weight_pairs(1))
    ]
    def column_start(b):
        return pl.multiple_of((2 * b + column) * own, own)

    first_row = pl.multiple_of(sp_at * block_rows, block_rows)
    first_loads = [
        pltpu.make_async_copy(source, target, first_sem.at[n])
        for n, (source, target) in enumerate(
            [
                (tables_hbm.at[:, :, pl.ds(first_row, block_rows)], tables),
                (out_weight_hbm, out_weight),
            ]
            + [
                (residual_hbm.at[pl.ds(column_start(b), own)], residual.at[b])
                for b in range(halves)
            ]
        )
    ]
    for load in first_loads + loads:
        load.start()

    group_width, _ = queries_ref.shape
    group = group_width // HEAD_DIM

    @pl.when(sp_at == 0)
    def _():
        near_keys[:WINDOW, :] = jnp.zeros((WINDOW, HEAD_DIM), near_keys.dtype)
        near_values[:, :WINDOW] = jnp.zeros((HEAD_DIM, WINDOW), near_values.dtype)

    @pl.when(sp_at == token_split - 1)
    def _():
        near_keys[WINDOW + block_rows :, :] = jnp.zeros((WINDOW, HEAD_DIM), near_keys.dtype)
        near_values[:, WINDOW + block_rows :] = jnp.zeros((HEAD_DIM, WINDOW), near_values.dtype)

    barrier = pltpu.get_barrier_semaphore()

    @pl.loop(1, token_split)
    def _(i):
        pl.semaphore_signal(
            barrier,
            inc=1,
            device_id=(flipped(sp_at, i, token_split), tp_at),
            device_id_type=MESH,
        )

    for partner in (pair, cross, diagonal):
        pl.semaphore_signal(barrier, inc=1, device_id=(sp_at, partner), device_id_type=MESH)

    first_loads[0].wait()
    quarter = HEAD_DIM // 4

    def turn(ref, base):
        pieces = []
        for n in range(2):
            cosine, sine = tables[2 * n], tables[2 * n + 1]
            start = base + 2 * n * quarter
            former = ref[start : start + quarter, :].astype(jnp.float32)
            latter = ref[start + quarter : start + 2 * quarter, :].astype(jnp.float32)
            pieces += [former * cosine - latter * sine, former * sine + latter * cosine]
        return pieces

    turned_keys = jnp.concatenate(turn(keys_ref, 0), axis=0)
    near_keys[WINDOW : WINDOW + block_rows, :] = turned_keys.T.astype(near_keys.dtype)
    near_values[:, WINDOW : WINDOW + block_rows] = values_ref[...]
    pl.semaphore_wait(barrier, token_split + 2)

    def halo(n, direction):
        lo = WINDOW if direction == 0 else block_rows
        to = WINDOW + block_rows if direction == 0 else 0
        there = sp_at - 1 if direction == 0 else sp_at + 1
        if n == 0:
            source, target = near_keys.at[lo : lo + WINDOW, :], near_keys.at[to : to + WINDOW, :]
        else:
            source, target = (
                near_values.at[:, lo : lo + WINDOW],
                near_values.at[:, to : to + WINDOW],
            )
        return pltpu.make_async_remote_copy(
            src_ref=source,
            dst_ref=target,
            send_sem=halo_send.at[direction, n],
            recv_sem=halo_recv.at[direction, n],
            device_id=(there, tp_at),
            device_id_type=MESH,
        )

    has_before = sp_at > 0
    has_after = sp_at < token_split - 1

    @pl.when(has_before)
    def _():
        halo(0, 0).start()
        halo(1, 0).start()

    @pl.when(has_after)
    def _():
        halo(0, 1).start()
        halo(1, 1).start()

    for share in shares[:4]:
        share.start()

    for h in range(group):
        for n, piece in enumerate(turn(queries_ref, h * HEAD_DIM)):
            start = h * HEAD_DIM + n * quarter
            turned[start : start + quarter, :] = piece.astype(turned.dtype)

    square = (block_rows, block_rows)
    before = lax.broadcasted_iota(jnp.int32, square, 0)
    after = lax.broadcasted_iota(jnp.int32, square, 1)
    earlier = (before < after) & (before // own == after // own)
    same_place = before == after
    ids_row = [ids_ref[k : k + 1, :] for k in range(TOPK)]
    ids_column = [
        jnp.sum(jnp.where(same_place, row, 0), axis=1, keepdims=True) for row in ids_row
    ]
    half_row = lax.broadcasted_iota(jnp.int32, (1, block_rows), 1) // (2 * own)
    codes, spots = [], []
    for k in range(TOPK):
        found = jnp.zeros(square, jnp.int32)
        for another in range(TOPK):
            found = found + ((ids_column[another] == ids_row[k]) & earlier).astype(jnp.int32)
        rank = jnp.sum(found, axis=0, keepdims=True)
        home = ids_row[k] // experts
        spots.append(home * rows + (ids_row[k] - home * experts) * capacity + rank)
        codes.append(ids_row[k] * rows + half_row * capacity + rank)

    def block_of(row, b):
        return row[:, b * own : (b + 1) * own]

    def column_block(row, b):
        return jnp.where(column == 0, block_of(row, 2 * b), block_of(row, 2 * b + 1))

    column_codes = [
        jnp.concatenate([column_block(code, b) for b in range(halves)], axis=1) for code in codes
    ]
    own_spots = [
        jnp.where(half == 0, column_block(spot, 0), column_block(spot, 1)) for spot in spots
    ]
    slot_at = lax.broadcasted_iota(jnp.int32, (rows, halves * own), 0)

    def chosen(at, expert):
        wanted = slot_at + (at * experts + expert) * rows
        return jnp.where(
            (column_codes[0] == wanted) | (column_codes[1] == wanted), 1.0, 0.0
        ).astype(jnp.bfloat16)

    def remote(stage, i, source, target, where):
        return pltpu.make_async_remote_copy(
            src_ref=source,
            dst_ref=target,
            send_sem=send.at[stage, i],
            recv_sem=recv.at[stage, i],
            device_id=where,
            device_id_type=MESH,
        )

    def partner_of(i):
        return flipped(sp_at, i, token_split)

    near = token_split // 2
    middle = lax.rem(lax.div(sp_at, near) + lax.div(sp_at, max(1, near // 2)), 2)

    def in_order(step):
        return flipped(step, middle * (near // 2) * lax.div(step, near), token_split)

    def along(i):
        there = partner_of(i)
        return remote(0, i, outgoing.at[there], arrived.at[i, half], (there, tp_at))

    def along_other(i):
        there = partner_of(i)
        return remote(1, i, outgoing_other.at[i], arrived.at[i, other], (there, tp_at))

    def over(i):
        piece = arrived.at[i, half]
        return remote(1, i, piece, piece, (sp_at, cross))

    def cross_back(i):
        return remote(2, i, part.at[i, other], from_cross.at[i], (sp_at, cross))

    def home_copy(i):
        there = partner_of(i)
        return remote(3, i, outgoing.at[there], back.at[sp_at], (there, tp_at))

    shared_over = pltpu.make_async_remote_copy(
        src_ref=shared_part.at[other],
        dst_ref=shared_got,
        send_sem=shared_sem.at[0],
        recv_sem=shared_sem.at[1],
        device_id=(sp_at, cross),
        device_id_type=MESH,
    )

    def weigh_work():
        square = (own, own)
        eye = lax.broadcasted_iota(jnp.int32, square, 0) == lax.broadcasted_iota(
            jnp.int32, square, 1
        )
        slot_of = lax.broadcasted_iota(jnp.int32, (own, token_split * rows), 1)
        weigh = jnp.zeros((own, token_split * rows), jnp.float32)
        for k in range(TOPK):
            spot = jnp.sum(jnp.where(eye, own_spots[k], 0), axis=1, keepdims=True)
            weight = jnp.sum(
                jnp.where(eye, weights_ref[k : k + 1, :], 0.0), axis=1, keepdims=True
            )
            weigh = jnp.where(slot_of == spot, weight, weigh)
        coarse = weigh.astype(jnp.bfloat16)
        weigh_ref[:own, :] = coarse
        weigh_ref[own:, :] = (weigh - coarse.astype(jnp.float32)).astype(jnp.bfloat16)

    weigh_work()

    key_at = lax.broadcasted_iota(jnp.int32, (3 * WINDOW, group * WINDOW), 0)
    query_at = lax.broadcasted_iota(jnp.int32, (3 * WINDOW, group * WINDOW), 1)
    near_enough = jnp.abs(key_at - WINDOW - query_at % WINDOW) <= WINDOW
    head_at = lax.broadcasted_iota(jnp.int32, (1, group * WINDOW), 1) // WINDOW
    sink = jnp.full((1, group * WINDOW), sinks_ref[0])
    for h in range(1, group):
        sink = jnp.where(head_at == h, sinks_ref[h], sink)
    blocks = block_rows // WINDOW
    total_rows = token_split * block_rows

    def attend(block):
        start = block * WINDOW
        query = jnp.concatenate(
            [
                turned[h * HEAD_DIM : (h + 1) * HEAD_DIM, start : start + WINDOW]
                for h in range(group)
            ],
            axis=1,
        )
        allowed = near_enough
        if block == 0:
            allowed = allowed & (key_at + (first_row - WINDOW) >= 0)
        if block == blocks - 1:
            allowed = allowed & (key_at + (first_row + start - WINDOW) < total_rows)
        scores = dot32(near_keys[start : start + 3 * WINDOW, :], query) * HEAD_DIM ** (-0.5)
        scores = jnp.where(allowed, scores, NEG_LARGE)
        highest = jnp.maximum(jnp.max(scores, axis=0, keepdims=True), sink)
        lifted = jnp.exp(scores - highest)
        below = jnp.sum(lifted, axis=0, keepdims=True) + jnp.exp(sink - highest)
        chances = (lifted * (1.0 / below)).astype(jnp.bfloat16)
        result = dot32(near_values[:, start : start + 3 * WINDOW], chances)
        heads = jnp.concatenate(
            [result[:, h * WINDOW : (h + 1) * WINDOW] for h in range(group)], axis=0
        )
        attended[start : start + WINDOW, :] = heads.T.astype(attended.dtype)

    for block in range(1, blocks - 1):
        attend(block)

    @pl.when(has_before)
    def _():
        halo(0, 1).wait_recv()
        halo(1, 1).wait_recv()

    attend(0)

    @pl.when(has_after)
    def _():
        halo(0, 0).wait_recv()
        halo(1, 0).wait_recv()

    if blocks > 1:
        attend(blocks - 1)

    def gather(n, b):
        partner = (cross, diagonal, pair)[n]
        start = pl.multiple_of((2 * b + lax.rem(partner, 2)) * own, own)
        return pltpu.make_async_remote_copy(
            src_ref=attended.at[pl.ds(start, own), :],
            dst_ref=gathered.at[tp_at, b],
            send_sem=gather_send.at[n, b],
            recv_sem=gather_recv.at[n, b],
            device_id=(sp_at, partner),
            device_id_type=MESH,
        )

    for n in range(3):
        for b in range(halves):
            gather(n, b).start()
    for b in range(halves):
        gathered[tp_at, b] = attended[pl.ds(column_start(b), own), :]
    for share in shares[4:]:
        share.start()
    for load in first_loads[1:]:
        load.wait()

    tile = min(width, 512)

    def projected(source, at):
        rows_at = pl.ds(pl.multiple_of(source * group_width, group_width), group_width)
        return dot32(
            gathered[source].reshape(halves * own, group_width), out_weight[rows_at, at]
        )

    @pl.loop(0, width // tile)
    def _(n):
        at = pl.ds(pl.multiple_of(n * tile, tile), tile)
        summed_rows[:, at] = projected(tp_at, at) + residual[:, :, at].reshape(
            halves * own, tile
        ).astype(jnp.float32)

    for n in range(3):
        for b in range(halves):
            gather(n, b).wait_recv()

    squares = jnp.zeros((halves * own, 1), jnp.float32)
    for n in range(width // tile):
        at = slice(n * tile, (n + 1) * tile)
        value = summed_rows[:, at]
        for source in (pair, cross, diagonal):
            value = value + projected(source, at)
        value = value.astype(mixed.dtype)
        mixed[:, :, at] = value.reshape(halves, own, tile)
        value = value.astype(jnp.float32)
        squares = squares + jnp.sum(value * value, axis=1, keepdims=True)
    scale_rows = lax.rsqrt(squares * (1.0 / width) + NORM_EPSILON)
    for n in range(width // tile):
        at = slice(n * tile, (n + 1) * tile)
        value = mixed[:, :, at].reshape(halves * own, tile).astype(jnp.float32)
        column_rows[:, at] = (value * scale_rows * gain_ref[:, at]).astype(column_rows.dtype)

    @pl.loop(1, token_split)
    def _(step):
        i = 1 + lax.rem(step - 1 + middle * (near - 1), token_split - 1)
        there = partner_of(i)
        outgoing[there] = dot32(chosen(there, half), column_rows[...]).astype(outgoing.dtype)
        along(i).start()

        @pl.when(i < near)
        def _():
            outgoing_other[i] = dot32(chosen(there, other), column_rows[...]).astype(
                outgoing_other.dtype
            )
            along_other(i).start()

    for e in range(experts):
        arrived[0, e] = dot32(chosen(sp_at, e), column_rows[...]).astype(arrived.dtype)

    def work(i):
        for e in range(experts):
            x = arrived[i, e]
            for p in range(2):
                hidden[e, :, p * hid : (p + 1) * hid] = silu_times(
                    dot32(x, gate[p, e]), dot32(x, up[p, e])
                ).astype(hidden.dtype)

        @pl.loop(0, width // tile)
        def _(n):
            at = pl.ds(pl.multiple_of(n * tile, tile), tile)
            results = [dot32(hidden[e], down[e, :, at]) for e in range(experts)]
            for b in range(halves):
                if capacity % 8 == 0 and rows == experts * capacity:
                    piece = jnp.concatenate(
                        [result[b * capacity : (b + 1) * capacity] for result in results], axis=0
                    )
                else:
                    piece = jnp.zeros((rows, tile), jnp.float32)
                    into = lax.broadcasted_iota(jnp.int32, (rows, rows), 0)
                    source = lax.broadcasted_iota(jnp.int32, (rows, rows), 1)
                    for e in range(experts):
                        rank = into - e * capacity
                        picked = (
                            (rank >= 0) & (rank < capacity) & (source == rank + b * capacity)
                        )
                        piece = piece + dot32(
                            jnp.where(picked, 1.0, 0.0).astype(jnp.bfloat16),
                            results[e].astype(jnp.bfloat16),
                        )
                part[i, b, :, at] = piece.astype(part.dtype)

    def forward(step):
        i = in_order(step)
        along(i).wait_recv()

        @pl.when(step >= near)
        def _():
            over(i).start()

    for n in range(3):
        loads[n].wait()
        shares[n].wait()
    shared_hidden = silu_times(
        dot32(column_rows[...], shared_gate[...]), dot32(column_rows[...], shared_up[...])
    ).astype(jnp.bfloat16)
    for n in range(width // tile):
        at = slice(n * tile, (n + 1) * tile)
        shared_part[:, :, at] = (
            dot32(shared_hidden, shared_down[:, at])
            .astype(shared_part.dtype)
            .reshape(halves, own, tile)
        )
    shared_over.start()
    for n in range(3, 6):
        loads[n].wait()
        shares[n].wait()

    @pl.loop(0, token_split + 1)
    def _(step):
        @pl.when(step < token_split)
        def _():
            i = in_order(step)

            @pl.when(step >= 1)
            def _():
                over(i).wait_recv()

            work(i)
            cross_back(i).start()

        @pl.when(step == 0)
        def _():
            forward(1)

        @pl.when(step >= 1)
        def _():
            i = in_order(step - 1)
            cross_back(i).wait_recv()
            summed = total(part[i, half], from_cross[i]).astype(back.dtype)

            @pl.when(step == 1)
            def _():
                back[sp_at] = summed

            @pl.when(step >= 2)
            def _():
                along(i).wait_send()
                outgoing[partner_of(i)] = summed
                home_copy(i).start()

        @pl.when(step + 2 < token_split)
        def _():
            forward(step + 2)

    shared_over.wait_recv()

    @pl.loop(1, token_split)
    def _(i):
        home_copy(i).wait_recv()

    for n in range(width // tile):
        at = slice(n * tile, (n + 1) * tile)
        routed = dot32(weigh_ref[...], back[:, :, at].reshape(token_split * rows, tile))
        out_ref[:, at] = (
            total(mixed[half, :, at], shared_part[half, :, at], shared_got[:, at])
            + routed[:own]
            + routed[own:]
        ).astype(out_ref.dtype)

    @pl.loop(0, token_split)
    def _(i):
        cross_back(i).wait_send()

    @pl.loop(1, token_split)
    def _(i):
        over(i).wait_send()
        home_copy(i).wait_send()

    shared_over.wait_send()
    for n in range(3):
        for b in range(halves):
            gather(n, b).wait_send()

    @pl.when(has_before)
    def _():
        halo(0, 0).wait_send()
        halo(1, 0).wait_send()

    @pl.when(has_after)
    def _():
        halo(0, 1).wait_send()
        halo(1, 1).wait_send()


def per_device(
    queries,
    keys,
    values,
    sinks,
    residual,
    out_weight,
    norm_gain,
    shared_gate,
    shared_up,
    shared_down,
    expert_ids,
    route_weights,
    expert_gate,
    expert_up,
    expert_down,
):
    token_split = lax.axis_size("sp")
    width_split = lax.axis_size("tp")
    experts, width, hid = expert_gate.shape
    block_rows, query_width = queries.shape
    if experts != 2 or width_split != 4 or keys.shape[1] != HEAD_DIM:
        raise ValueError("unsupported split")
    own = route_weights.shape[0]
    capacity = max(2, 2 * own * TOPK // (experts * token_split))
    rows = -(-experts * capacity // 16) * 16
    shared_hid = shared_gate.shape[1]
    kind = queries.dtype
    chunk = (rows, width)
    hbm = pl.BlockSpec(memory_space=pltpu.HBM)
    dma = pltpu.SemaphoreType.DMA
    wide_rows = block_rows + 2 * WINDOW
    return pl.pallas_call(
        functools.partial(layer_kernel, token_split, capacity),
        out_shape=jax.ShapeDtypeStruct((own, width), kind),
        in_specs=[pl.BlockSpec(memory_space=pltpu.SMEM)] + [VMEM] * 6 + [hbm] * 9,
        out_specs=VMEM,
        scratch_shapes=[
            pltpu.VMEM((4, HEAD_DIM // 4, block_rows), jnp.float32),
            pltpu.VMEM((2, own, width), kind),
            pltpu.VMEM(out_weight.shape, kind),
            pltpu.VMEM((query_width, block_rows), kind),
            pltpu.VMEM((wide_rows, HEAD_DIM), kind),
            pltpu.VMEM((HEAD_DIM, wide_rows), kind),
            pltpu.VMEM((block_rows, query_width), kind),
            pltpu.VMEM((width_split, 2, own, query_width), kind),
            pltpu.VMEM((2 * own, width), jnp.float32),
            pltpu.VMEM((2, own, width), kind),
            pltpu.VMEM((width, 2 * shared_hid), kind),
            pltpu.VMEM((width, 2 * shared_hid), kind),
            pltpu.VMEM((2 * shared_hid, width), kind),
            pltpu.VMEM((2, experts, width, hid), kind),
            pltpu.VMEM((2, experts, width, hid), kind),
            pltpu.VMEM((experts, 2 * hid, width), kind),
            pltpu.VMEM((2 * own, width), kind),
            pltpu.VMEM((experts, rows, 2 * hid), kind),
            pltpu.VMEM((2 * own, token_split * rows), kind),
            pltpu.VMEM((token_split,) + chunk, kind),
            pltpu.VMEM((token_split // 2,) + chunk, kind),
            pltpu.VMEM((token_split, experts) + chunk, kind),
            pltpu.VMEM((token_split, 2) + chunk, kind),
            pltpu.VMEM((token_split,) + chunk, kind),
            pltpu.VMEM((token_split,) + chunk, kind),
            pltpu.VMEM((2, own, width), kind),
            pltpu.VMEM((own, width), kind),
            dma((6,)),
            dma((6,)),
            dma((6,)),
            dma((4, token_split)),
            dma((4, token_split)),
            dma((2,)),
            dma((4,)),
            dma((2, 2)),
            dma((2, 2)),
            dma((3, 2)),
            dma((3, 2)),
        ],
        compiler_params=pltpu.CompilerParams(
            collective_id=1, has_side_effects=True, vmem_limit_bytes=VMEM_LIMIT
        ),
        name="layer",
    )(
        sinks,
        queries.T,
        keys.T,
        values.T,
        norm_gain.reshape(1, width),
        expert_ids.T,
        route_weights.T,
        jnp.asarray(turn_tables(token_split * block_rows)),
        residual,
        out_weight,
        shared_gate,
        shared_up,
        shared_down,
        expert_gate,
        expert_up,
        expert_down,
    )


def solution(mesh):
    placed = (
        P("sp", "tp"),
        P("sp", "tp"),
        P("sp", "tp"),
        P("tp"),
        P("sp", None),
        P(),
        P(),
        P(None, "tp"),
        P(None, "tp"),
        P("tp", None),
        P("sp", None),
        P(("sp", "tp"), None),
        P("sp", None, "tp"),
        P("sp", None, "tp"),
        P("sp", "tp", None),
    )
    return jax.shard_map(
        per_device, mesh=mesh, in_specs=placed, out_specs=P(("sp", "tp"), None), check_vma=False
    )
```

```python
import jax
import jax.numpy as jnp
import numpy as np
from jax import lax
from jax.experimental import pallas as pl
from jax.experimental.pallas import tpu as pltpu
from jax.sharding import PartitionSpec as P
import functools

MESH = pl.DeviceIdType.MESH
VMEM = pl.BlockSpec(memory_space=pltpu.VMEM)
VMEM_LIMIT = 62 * 1024 * 1024

HEAD_DIM = 64
WINDOW = 128
GRID_W = 64
TOPK = 2


ROPE_BASE = 10000.0
NEG_LARGE = -1e30
NORM_EPSILON = 1e-06


def turn_tables(total_rows):
    halfway = HEAD_DIM // 2
    spectrum = np.float32(ROPE_BASE) ** (
        -np.arange(0, halfway, 2, dtype=np.float32) / np.float32(halfway)
    )
    places = np.arange(total_rows)
    tables = []
    for offsets in (places // GRID_W, places % GRID_W):
        angles = spectrum[:, None].astype(np.float32) * offsets.astype(np.float32)[None, :]
        tables += [np.cos(angles), np.sin(angles)]
    return np.stack(tables).astype(np.float32)


def flipped(a, b, size):
    total, bit = 0, 1
    while bit < size:
        total = total + (lax.rem(lax.div(a, bit) + lax.div(b, bit), 2)) * bit
        bit *= 2
    return total


def dot32(a, b):
    return jnp.dot(a, b, preferred_element_type=jnp.float32)


def total(*terms):
    value = terms[0].astype(jnp.float32)
    for term in terms[1:]:
        value = value + term.astype(jnp.float32)
    return value


def silu_times(gate_values, up_values):
    return gate_values / (1.0 + jnp.exp(-gate_values)) * up_values


def layer_kernel(
    token_split,
    capacity,
    sinks_ref,
    queries_ref,
    keys_ref,
    values_ref,
    gain_ref,
    ids_ref,
    weights_ref,
    tables_hbm,
    residual_hbm,
    out_weight_hbm,
    shared_gate_hbm,
    shared_up_hbm,
    shared_down_hbm,
    gate_hbm,
    up_hbm,
    down_hbm,
    out_ref,
    tables,
    residual,
    out_weight,
    turned,
    near_keys,
    near_values,
    attended,
    gathered,
    summed_rows,
    mixed,
    shared_gate,
    shared_up,
    shared_down,
    gate,
    up,
    down,
    column_rows,
    hidden,
    weigh_ref,
    outgoing,
    outgoing_other,
    arrived,
    part,
    from_cross,
    back,
    shared_part,
    shared_got,
    load_sem,
    weight_send,
    weight_recv,
    send,
    recv,
    shared_sem,
    first_sem,
    halo_send,
    halo_recv,
    gather_send,
    gather_recv,
):
    _, experts, rows, width = arrived.shape
    hid = gate.shape[3]
    shared_hid = shared_down_hbm.shape[0]
    own = out_ref.shape[0]
    block_rows = queries_ref.shape[1]
    halves = experts
    sp_at = lax.axis_index("sp")
    tp_at = lax.axis_index("tp")
    column = lax.rem(tp_at, 2)
    half = lax.div(tp_at, 2)
    other = 1 - half
    pair = 2 * half + 1 - column
    cross = 2 * other + column
    diagonal = 2 * other + 1 - column

    def weight_pairs(which):
        side = pl.ds(which * shared_hid, shared_hid)
        return (
            (shared_gate_hbm, shared_gate.at[:, side]),
            (shared_up_hbm, shared_up.at[:, side]),
            (shared_down_hbm, shared_down.at[side, :]),
            (gate_hbm, gate.at[which]),
            (up_hbm, up.at[which]),
            (down_hbm, down.at[:, pl.ds(which * hid, hid), :]),
        )

    loads = [
        pltpu.make_async_copy(source, target, load_sem.at[n])
        for n, (source, target) in enumerate(weight_pairs(0))
    ]
    shares = [
        pltpu.make_async_remote_copy(
            src_ref=source,
            dst_ref=target,
            send_sem=weight_send.at[n],
            recv_sem=weight_recv.at[n],
            device_id=(sp_at, pair),
            device_id_type=MESH,
        )
        for n, (source, target) in enumerate(weight_pairs(1))
    ]
    def column_start(b):
        return pl.multiple_of((2 * b + column) * own, own)

    first_row = pl.multiple_of(sp_at * block_rows, block_rows)
    first_loads = [
        pltpu.make_async_copy(source, target, first_sem.at[n])
        for n, (source, target) in enumerate(
            [
                (tables_hbm.at[:, :, pl.ds(first_row, block_rows)], tables),
                (out_weight_hbm, out_weight),
            ]
            + [
                (residual_hbm.at[pl.ds(column_start(b), own)], residual.at[b])
                for b in range(halves)
            ]
        )
    ]
    for load in first_loads + loads:
        load.start()

    group_width, _ = queries_ref.shape
    group = group_width // HEAD_DIM

    @pl.when(sp_at == 0)
    def _():
        near_keys[:WINDOW, :] = jnp.zeros((WINDOW, HEAD_DIM), near_keys.dtype)
        near_values[:, :WINDOW] = jnp.zeros((HEAD_DIM, WINDOW), near_values.dtype)

    @pl.when(sp_at == token_split - 1)
    def _():
        near_keys[WINDOW + block_rows :, :] = jnp.zeros((WINDOW, HEAD_DIM), near_keys.dtype)
        near_values[:, WINDOW + block_rows :] = jnp.zeros((HEAD_DIM, WINDOW), near_values.dtype)

    barrier = pltpu.get_barrier_semaphore()

    @pl.loop(1, token_split)
    def _(i):
        pl.semaphore_signal(
            barrier,
            inc=1,
            device_id=(flipped(sp_at, i, token_split), tp_at),
            device_id_type=MESH,
        )

    for partner in (pair, cross, diagonal):
        pl.semaphore_signal(barrier, inc=1, device_id=(sp_at, partner), device_id_type=MESH)

    first_loads[0].wait()
    quarter = HEAD_DIM // 4

    def turn(ref, base):
        pieces = []
        for n in range(2):
            cosine, sine = tables[2 * n], tables[2 * n + 1]
            start = base + 2 * n * quarter
            former = ref[start : start + quarter, :].astype(jnp.float32)
            latter = ref[start + quarter : start + 2 * quarter, :].astype(jnp.float32)
            pieces += [former * cosine - latter * sine, former * sine + latter * cosine]
        return pieces

    turned_keys = jnp.concatenate(turn(keys_ref, 0), axis=0)
    near_keys[WINDOW : WINDOW + block_rows, :] = turned_keys.T.astype(near_keys.dtype)
    near_values[:, WINDOW : WINDOW + block_rows] = values_ref[...]
    pl.semaphore_wait(barrier, token_split + 2)

    def halo(n, direction):
        lo = WINDOW if direction == 0 else block_rows
        to = WINDOW + block_rows if direction == 0 else 0
        there = sp_at - 1 if direction == 0 else sp_at + 1
        if n == 0:
            source, target = near_keys.at[lo : lo + WINDOW, :], near_keys.at[to : to + WINDOW, :]
        else:
            source, target = (
                near_values.at[:, lo : lo + WINDOW],
                near_values.at[:, to : to + WINDOW],
            )
        return pltpu.make_async_remote_copy(
            src_ref=source,
            dst_ref=target,
            send_sem=halo_send.at[direction, n],
            recv_sem=halo_recv.at[direction, n],
            device_id=(there, tp_at),
            device_id_type=MESH,
        )

    has_before = sp_at > 0
    has_after = sp_at < token_split - 1

    @pl.when(has_before)
    def _():
        halo(0, 0).start()
        halo(1, 0).start()

    @pl.when(has_after)
    def _():
        halo(0, 1).start()
        halo(1, 1).start()

    for share in shares[:4]:
        share.start()

    for h in range(group):
        for n, piece in enumerate(turn(queries_ref, h * HEAD_DIM)):
            start = h * HEAD_DIM + n * quarter
            turned[start : start + quarter, :] = piece.astype(turned.dtype)

    square = (block_rows, block_rows)
    before = lax.broadcasted_iota(jnp.int32, square, 0)
    after = lax.broadcasted_iota(jnp.int32, square, 1)
    earlier = (before < after) & (before // own == after // own)
    same_place = before == after
    ids_row = [ids_ref[k : k + 1, :] for k in range(TOPK)]
    ids_column = [
        jnp.sum(jnp.where(same_place, row, 0), axis=1, keepdims=True) for row in ids_row
    ]
    half_row = lax.broadcasted_iota(jnp.int32, (1, block_rows), 1) // (2 * own)
    codes, spots = [], []
    for k in range(TOPK):
        found = jnp.zeros(square, jnp.int32)
        for another in range(TOPK):
            found = found + ((ids_column[another] == ids_row[k]) & earlier).astype(jnp.int32)
        rank = jnp.sum(found, axis=0, keepdims=True)
        home = ids_row[k] // experts
        spots.append(home * rows + (ids_row[k] - home * experts) * capacity + rank)
        codes.append(ids_row[k] * rows + half_row * capacity + rank)

    def block_of(row, b):
        return row[:, b * own : (b + 1) * own]

    def column_block(row, b):
        return jnp.where(column == 0, block_of(row, 2 * b), block_of(row, 2 * b + 1))

    column_codes = [
        jnp.concatenate([column_block(code, b) for b in range(halves)], axis=1) for code in codes
    ]
    own_spots = [
        jnp.where(half == 0, column_block(spot, 0), column_block(spot, 1)) for spot in spots
    ]
    slot_at = lax.broadcasted_iota(jnp.int32, (rows, halves * own), 0)

    def chosen(at, expert):
        wanted = slot_at + (at * experts + expert) * rows
        return jnp.where(
            (column_codes[0] == wanted) | (column_codes[1] == wanted), 1.0, 0.0
        ).astype(jnp.bfloat16)

    def remote(stage, i, source, target, where):
        return pltpu.make_async_remote_copy(
            src_ref=source,
            dst_ref=target,
            send_sem=send.at[stage, i],
            recv_sem=recv.at[stage, i],
            device_id=where,
            device_id_type=MESH,
        )

    def partner_of(i):
        return flipped(sp_at, i, token_split)

    near = token_split // 2
    middle = lax.rem(lax.div(sp_at, near) + lax.div(sp_at, max(1, near // 2)), 2)

    def in_order(step):
        last = token_split - 2
        step = jnp.where(step < 2, step, 2 + lax.rem(step + near - 4 + last, last))
        return flipped(step, middle * (near // 2) * lax.div(step, near), token_split)

    def along(i):
        there = partner_of(i)
        return remote(0, i, outgoing.at[there], arrived.at[i, half], (there, tp_at))

    def along_other(i):
        there = partner_of(i)
        return remote(1, i, outgoing_other.at[i], arrived.at[i, other], (there, tp_at))

    def over(i):
        piece = arrived.at[i, half]
        return remote(1, i, piece, piece, (sp_at, cross))

    def cross_back(i):
        return remote(2, i, part.at[i, other], from_cross.at[i], (sp_at, cross))

    def home_copy(i):
        there = partner_of(i)
        return remote(3, i, outgoing.at[there], back.at[sp_at], (there, tp_at))

    shared_over = pltpu.make_async_remote_copy(
        src_ref=shared_part.at[other],
        dst_ref=shared_got,
        send_sem=shared_sem.at[0],
        recv_sem=shared_sem.at[1],
        device_id=(sp_at, cross),
        device_id_type=MESH,
    )

    def weigh_work():
        square = (own, own)
        eye = lax.broadcasted_iota(jnp.int32, square, 0) == lax.broadcasted_iota(
            jnp.int32, square, 1
        )
        slot_of = lax.broadcasted_iota(jnp.int32, (own, token_split * rows), 1)
        weigh = jnp.zeros((own, token_split * rows), jnp.float32)
        for k in range(TOPK):
            spot = jnp.sum(jnp.where(eye, own_spots[k], 0), axis=1, keepdims=True)
            weight = jnp.sum(
                jnp.where(eye, weights_ref[k : k + 1, :], 0.0), axis=1, keepdims=True
            )
            weigh = jnp.where(slot_of == spot, weight, weigh)
        coarse = weigh.astype(jnp.bfloat16)
        weigh_ref[:own, :] = coarse
        weigh_ref[own:, :] = (weigh - coarse.astype(jnp.float32)).astype(jnp.bfloat16)

    weigh_work()

    key_at = lax.broadcasted_iota(jnp.int32, (3 * WINDOW, group * WINDOW), 0)
    query_at = lax.broadcasted_iota(jnp.int32, (3 * WINDOW, group * WINDOW), 1)
    near_enough = jnp.abs(key_at - WINDOW - query_at % WINDOW) <= WINDOW
    head_at = lax.broadcasted_iota(jnp.int32, (1, group * WINDOW), 1) // WINDOW
    sink = jnp.full((1, group * WINDOW), sinks_ref[0])
    for h in range(1, group):
        sink = jnp.where(head_at == h, sinks_ref[h], sink)
    blocks = block_rows // WINDOW
    total_rows = token_split * block_rows

    def attend(block):
        start = block * WINDOW
        query = jnp.concatenate(
            [
                turned[h * HEAD_DIM : (h + 1) * HEAD_DIM, start : start + WINDOW]
                for h in range(group)
            ],
            axis=1,
        )
        allowed = near_enough
        if block == 0:
            allowed = allowed & (key_at + (first_row - WINDOW) >= 0)
        if block == blocks - 1:
            allowed = allowed & (key_at + (first_row + start - WINDOW) < total_rows)
        scores = dot32(near_keys[start : start + 3 * WINDOW, :], query) * HEAD_DIM ** (-0.5)
        scores = jnp.where(allowed, scores, NEG_LARGE)
        highest = jnp.maximum(jnp.max(scores, axis=0, keepdims=True), sink)
        lifted = jnp.exp(scores - highest)
        below = jnp.sum(lifted, axis=0, keepdims=True) + jnp.exp(sink - highest)
        chances = (lifted * (1.0 / below)).astype(jnp.bfloat16)
        result = dot32(near_values[:, start : start + 3 * WINDOW], chances)
        heads = jnp.concatenate(
            [result[:, h * WINDOW : (h + 1) * WINDOW] for h in range(group)], axis=0
        )
        attended[start : start + WINDOW, :] = heads.T.astype(attended.dtype)

    for block in range(1, blocks - 1):
        attend(block)

    @pl.when(has_before)
    def _():
        halo(0, 1).wait_recv()
        halo(1, 1).wait_recv()

    attend(0)

    @pl.when(has_after)
    def _():
        halo(0, 0).wait_recv()
        halo(1, 0).wait_recv()

    if blocks > 1:
        attend(blocks - 1)

    def gather(n, b):
        partner = (cross, diagonal, pair)[n]
        start = pl.multiple_of((2 * b + lax.rem(partner, 2)) * own, own)
        return pltpu.make_async_remote_copy(
            src_ref=attended.at[pl.ds(start, own), :],
            dst_ref=gathered.at[tp_at, b],
            send_sem=gather_send.at[n, b],
            recv_sem=gather_recv.at[n, b],
            device_id=(sp_at, partner),
            device_id_type=MESH,
        )

    for n in range(3):
        for b in range(halves):
            gather(n, b).start()
    for b in range(halves):
        gathered[tp_at, b] = attended[pl.ds(column_start(b), own), :]
    for share in shares[4:]:
        share.start()
    for load in first_loads[1:]:
        load.wait()

    tile = min(width, 512)

    def projected(source, at):
        rows_at = pl.ds(pl.multiple_of(source * group_width, group_width), group_width)
        return dot32(
            gathered[source].reshape(halves * own, group_width), out_weight[rows_at, at]
        )

    @pl.loop(0, width // tile)
    def _(n):
        at = pl.ds(pl.multiple_of(n * tile, tile), tile)
        summed_rows[:, at] = projected(tp_at, at) + residual[:, :, at].reshape(
            halves * own, tile
        ).astype(jnp.float32)

    for n in range(3):
        for b in range(halves):
            gather(n, b).wait_recv()

    squares = jnp.zeros((halves * own, 1), jnp.float32)
    for n in range(width // tile):
        at = slice(n * tile, (n + 1) * tile)
        value = summed_rows[:, at]
        for source in (pair, cross, diagonal):
            value = value + projected(source, at)
        value = value.astype(mixed.dtype)
        mixed[:, :, at] = value.reshape(halves, own, tile)
        value = value.astype(jnp.float32)
        squares = squares + jnp.sum(value * value, axis=1, keepdims=True)
    scale_rows = lax.rsqrt(squares * (1.0 / width) + NORM_EPSILON)
    for n in range(width // tile):
        at = slice(n * tile, (n + 1) * tile)
        value = mixed[:, :, at].reshape(halves * own, tile).astype(jnp.float32)
        column_rows[:, at] = (value * scale_rows * gain_ref[:, at]).astype(column_rows.dtype)

    @pl.loop(1, token_split)
    def _(step):
        i = 1 + lax.rem(step - 1 + middle * (near - 1), token_split - 1)
        there = partner_of(i)
        outgoing[there] = dot32(chosen(there, half), column_rows[...]).astype(outgoing.dtype)
        along(i).start()

        @pl.when(i < near)
        def _():
            outgoing_other[i] = dot32(chosen(there, other), column_rows[...]).astype(
                outgoing_other.dtype
            )
            along_other(i).start()

    for e in range(experts):
        arrived[0, e] = dot32(chosen(sp_at, e), column_rows[...]).astype(arrived.dtype)

    def work(i):
        for e in range(experts):
            x = arrived[i, e]
            for p in range(2):
                hidden[e, :, p * hid : (p + 1) * hid] = silu_times(
                    dot32(x, gate[p, e]), dot32(x, up[p, e])
                ).astype(hidden.dtype)

        @pl.loop(0, width // tile)
        def _(n):
            at = pl.ds(pl.multiple_of(n * tile, tile), tile)
            results = [dot32(hidden[e], down[e, :, at]) for e in range(experts)]
            for b in range(halves):
                if capacity % 8 == 0 and rows == experts * capacity:
                    piece = jnp.concatenate(
                        [result[b * capacity : (b + 1) * capacity] for result in results], axis=0
                    )
                else:
                    piece = jnp.zeros((rows, tile), jnp.float32)
                    into = lax.broadcasted_iota(jnp.int32, (rows, rows), 0)
                    source = lax.broadcasted_iota(jnp.int32, (rows, rows), 1)
                    for e in range(experts):
                        rank = into - e * capacity
                        picked = (
                            (rank >= 0) & (rank < capacity) & (source == rank + b * capacity)
                        )
                        piece = piece + dot32(
                            jnp.where(picked, 1.0, 0.0).astype(jnp.bfloat16),
                            results[e].astype(jnp.bfloat16),
                        )
                part[i, b, :, at] = piece.astype(part.dtype)

    def forward(step):
        i = in_order(step)
        along(i).wait_recv()

        @pl.when(i >= near)
        def _():
            over(i).start()

    for n in range(3):
        loads[n].wait()
        shares[n].wait()
    shared_hidden = silu_times(
        dot32(column_rows[...], shared_gate[...]), dot32(column_rows[...], shared_up[...])
    ).astype(jnp.bfloat16)
    for n in range(width // tile):
        at = slice(n * tile, (n + 1) * tile)
        shared_part[:, :, at] = (
            dot32(shared_hidden, shared_down[:, at])
            .astype(shared_part.dtype)
            .reshape(halves, own, tile)
        )
    shared_over.start()
    for n in range(3, 6):
        loads[n].wait()
        shares[n].wait()

    @pl.loop(0, token_split + 1)
    def _(step):
        @pl.when(step < token_split)
        def _():
            i = in_order(step)

            @pl.when(step >= 1)
            def _():
                over(i).wait_recv()

            work(i)
            cross_back(i).start()

        @pl.when(step == 0)
        def _():
            forward(1)

        @pl.when(step >= 1)
        def _():
            i = in_order(step - 1)
            cross_back(i).wait_recv()
            summed = total(part[i, half], from_cross[i]).astype(back.dtype)

            @pl.when(step == 1)
            def _():
                back[sp_at] = summed

            @pl.when(step >= 2)
            def _():
                along(i).wait_send()
                outgoing[partner_of(i)] = summed
                home_copy(i).start()

        @pl.when(step + 2 < token_split)
        def _():
            forward(step + 2)

    shared_over.wait_recv()

    @pl.loop(1, token_split)
    def _(i):
        home_copy(i).wait_recv()

    for n in range(width // tile):
        at = slice(n * tile, (n + 1) * tile)
        routed = dot32(weigh_ref[...], back[:, :, at].reshape(token_split * rows, tile))
        out_ref[:, at] = (
            total(mixed[half, :, at], shared_part[half, :, at], shared_got[:, at])
            + routed[:own]
            + routed[own:]
        ).astype(out_ref.dtype)

    @pl.loop(0, token_split)
    def _(i):
        cross_back(i).wait_send()

    @pl.loop(1, token_split)
    def _(i):
        over(i).wait_send()
        home_copy(i).wait_send()

    shared_over.wait_send()
    for n in range(3):
        for b in range(halves):
            gather(n, b).wait_send()

    @pl.when(has_before)
    def _():
        halo(0, 0).wait_send()
        halo(1, 0).wait_send()

    @pl.when(has_after)
    def _():
        halo(0, 1).wait_send()
        halo(1, 1).wait_send()


def per_device(
    queries,
    keys,
    values,
    sinks,
    residual,
    out_weight,
    norm_gain,
    shared_gate,
    shared_up,
    shared_down,
    expert_ids,
    route_weights,
    expert_gate,
    expert_up,
    expert_down,
):
    token_split = lax.axis_size("sp")
    width_split = lax.axis_size("tp")
    experts, width, hid = expert_gate.shape
    block_rows, query_width = queries.shape
    if experts != 2 or width_split != 4 or keys.shape[1] != HEAD_DIM:
        raise ValueError("unsupported split")
    own = route_weights.shape[0]
    capacity = max(2, 2 * own * TOPK // (experts * token_split))
    rows = -(-experts * capacity // 16) * 16
    shared_hid = shared_gate.shape[1]
    kind = queries.dtype
    chunk = (rows, width)
    hbm = pl.BlockSpec(memory_space=pltpu.HBM)
    dma = pltpu.SemaphoreType.DMA
    wide_rows = block_rows + 2 * WINDOW
    return pl.pallas_call(
        functools.partial(layer_kernel, token_split, capacity),
        out_shape=jax.ShapeDtypeStruct((own, width), kind),
        in_specs=[pl.BlockSpec(memory_space=pltpu.SMEM)] + [VMEM] * 6 + [hbm] * 9,
        out_specs=VMEM,
        scratch_shapes=[
            pltpu.VMEM((4, HEAD_DIM // 4, block_rows), jnp.float32),
            pltpu.VMEM((2, own, width), kind),
            pltpu.VMEM(out_weight.shape, kind),
            pltpu.VMEM((query_width, block_rows), kind),
            pltpu.VMEM((wide_rows, HEAD_DIM), kind),
            pltpu.VMEM((HEAD_DIM, wide_rows), kind),
            pltpu.VMEM((block_rows, query_width), kind),
            pltpu.VMEM((width_split, 2, own, query_width), kind),
            pltpu.VMEM((2 * own, width), jnp.float32),
            pltpu.VMEM((2, own, width), kind),
            pltpu.VMEM((width, 2 * shared_hid), kind),
            pltpu.VMEM((width, 2 * shared_hid), kind),
            pltpu.VMEM((2 * shared_hid, width), kind),
            pltpu.VMEM((2, experts, width, hid), kind),
            pltpu.VMEM((2, experts, width, hid), kind),
            pltpu.VMEM((experts, 2 * hid, width), kind),
            pltpu.VMEM((2 * own, width), kind),
            pltpu.VMEM((experts, rows, 2 * hid), kind),
            pltpu.VMEM((2 * own, token_split * rows), kind),
            pltpu.VMEM((token_split,) + chunk, kind),
            pltpu.VMEM((token_split // 2,) + chunk, kind),
            pltpu.VMEM((token_split, experts) + chunk, kind),
            pltpu.VMEM((token_split, 2) + chunk, kind),
            pltpu.VMEM((token_split,) + chunk, kind),
            pltpu.VMEM((token_split,) + chunk, kind),
            pltpu.VMEM((2, own, width), kind),
            pltpu.VMEM((own, width), kind),
            dma((6,)),
            dma((6,)),
            dma((6,)),
            dma((4, token_split)),
            dma((4, token_split)),
            dma((2,)),
            dma((4,)),
            dma((2, 2)),
            dma((2, 2)),
            dma((3, 2)),
            dma((3, 2)),
        ],
        compiler_params=pltpu.CompilerParams(
            collective_id=1, has_side_effects=True, vmem_limit_bytes=VMEM_LIMIT
        ),
        name="layer",
    )(
        sinks,
        queries.T,
        keys.T,
        values.T,
        norm_gain.reshape(1, width),
        expert_ids.T,
        route_weights.T,
        jnp.asarray(turn_tables(token_split * block_rows)),
        residual,
        out_weight,
        shared_gate,
        shared_up,
        shared_down,
        expert_gate,
        expert_up,
        expert_down,
    )


def solution(mesh):
    placed = (
        P("sp", "tp"),
        P("sp", "tp"),
        P("sp", "tp"),
        P("tp"),
        P("sp", None),
        P(),
        P(),
        P(None, "tp"),
        P(None, "tp"),
        P("tp", None),
        P("sp", None),
        P(("sp", "tp"), None),
        P("sp", None, "tp"),
        P("sp", None, "tp"),
        P("sp", "tp", None),
    )
    return jax.shard_map(
        per_device, mesh=mesh, in_specs=placed, out_specs=P(("sp", "tp"), None), check_vma=False
    )
```

```python
import jax
import jax.numpy as jnp
import numpy as np
from jax import lax
from jax.experimental import pallas as pl
from jax.experimental.pallas import tpu as pltpu
from jax.sharding import PartitionSpec as P
import functools

MESH = pl.DeviceIdType.MESH
VMEM = pl.BlockSpec(memory_space=pltpu.VMEM)
VMEM_LIMIT = 62 * 1024 * 1024

HEAD_DIM = 64
WINDOW = 128
GRID_W = 64
TOPK = 2


ROPE_BASE = 10000.0
NEG_LARGE = -1e30
NORM_EPSILON = 1e-06


def turn_tables(total_rows):
    halfway = HEAD_DIM // 2
    spectrum = np.float32(ROPE_BASE) ** (
        -np.arange(0, halfway, 2, dtype=np.float32) / np.float32(halfway)
    )
    places = np.arange(total_rows)
    tables = []
    for offsets in (places // GRID_W, places % GRID_W):
        angles = spectrum[:, None].astype(np.float32) * offsets.astype(np.float32)[None, :]
        tables += [np.cos(angles), np.sin(angles)]
    return np.stack(tables).astype(np.float32)


def flipped(a, b, size):
    total, bit = 0, 1
    while bit < size:
        total = total + (lax.rem(lax.div(a, bit) + lax.div(b, bit), 2)) * bit
        bit *= 2
    return total


def dot32(a, b):
    return jnp.dot(a, b, preferred_element_type=jnp.float32)


def total(*terms):
    value = terms[0].astype(jnp.float32)
    for term in terms[1:]:
        value = value + term.astype(jnp.float32)
    return value


def silu_times(gate_values, up_values):
    return gate_values / (1.0 + jnp.exp(-gate_values)) * up_values


def layer_kernel(
    token_split,
    capacity,
    sinks_ref,
    queries_ref,
    keys_ref,
    values_ref,
    gain_ref,
    ids_ref,
    weights_ref,
    tables_hbm,
    residual_hbm,
    out_weight_hbm,
    shared_gate_hbm,
    shared_up_hbm,
    shared_down_hbm,
    gate_hbm,
    up_hbm,
    down_hbm,
    out_ref,
    tables,
    residual,
    out_weight,
    turned,
    near_keys,
    near_values,
    attended,
    gathered,
    summed_rows,
    mixed,
    shared_gate,
    shared_up,
    shared_down,
    gate,
    up,
    down,
    column_rows,
    hidden,
    weigh_ref,
    outgoing,
    outgoing_other,
    arrived,
    part,
    from_cross,
    back,
    shared_part,
    shared_got,
    load_sem,
    weight_send,
    weight_recv,
    send,
    recv,
    shared_sem,
    first_sem,
    halo_send,
    halo_recv,
    gather_send,
    gather_recv,
):
    _, experts, rows, width = arrived.shape
    hid = gate.shape[3]
    shared_hid = shared_down_hbm.shape[0]
    own = out_ref.shape[0]
    block_rows = queries_ref.shape[1]
    halves = experts
    sp_at = lax.axis_index("sp")
    tp_at = lax.axis_index("tp")
    column = lax.rem(tp_at, 2)
    half = lax.div(tp_at, 2)
    other = 1 - half
    pair = 2 * half + 1 - column
    cross = 2 * other + column
    diagonal = 2 * other + 1 - column

    def weight_pairs(which):
        side = pl.ds(which * shared_hid, shared_hid)
        return (
            (shared_gate_hbm, shared_gate.at[:, side]),
            (shared_up_hbm, shared_up.at[:, side]),
            (shared_down_hbm, shared_down.at[side, :]),
            (gate_hbm, gate.at[which]),
            (up_hbm, up.at[which]),
            (down_hbm, down.at[:, pl.ds(which * hid, hid), :]),
        )

    loads = [
        pltpu.make_async_copy(source, target, load_sem.at[n])
        for n, (source, target) in enumerate(weight_pairs(0))
    ]
    shares = [
        pltpu.make_async_remote_copy(
            src_ref=source,
            dst_ref=target,
            send_sem=weight_send.at[n],
            recv_sem=weight_recv.at[n],
            device_id=(sp_at, pair),
            device_id_type=MESH,
        )
        for n, (source, target) in enumerate(weight_pairs(1))
    ]
    def column_start(b):
        return pl.multiple_of((2 * b + column) * own, own)

    first_row = pl.multiple_of(sp_at * block_rows, block_rows)
    first_loads = [
        pltpu.make_async_copy(source, target, first_sem.at[n])
        for n, (source, target) in enumerate(
            [
                (tables_hbm.at[:, :, pl.ds(first_row, block_rows)], tables),
                (out_weight_hbm, out_weight),
            ]
            + [
                (residual_hbm.at[pl.ds(column_start(b), own)], residual.at[b])
                for b in range(halves)
            ]
        )
    ]
    for load in first_loads + loads:
        load.start()

    group_width, _ = queries_ref.shape
    group = group_width // HEAD_DIM

    @pl.when(sp_at == 0)
    def _():
        near_keys[:WINDOW, :] = jnp.zeros((WINDOW, HEAD_DIM), near_keys.dtype)
        near_values[:, :WINDOW] = jnp.zeros((HEAD_DIM, WINDOW), near_values.dtype)

    @pl.when(sp_at == token_split - 1)
    def _():
        near_keys[WINDOW + block_rows :, :] = jnp.zeros((WINDOW, HEAD_DIM), near_keys.dtype)
        near_values[:, WINDOW + block_rows :] = jnp.zeros((HEAD_DIM, WINDOW), near_values.dtype)

    barrier = pltpu.get_barrier_semaphore()

    @pl.loop(1, token_split)
    def _(i):
        pl.semaphore_signal(
            barrier,
            inc=1,
            device_id=(flipped(sp_at, i, token_split), tp_at),
            device_id_type=MESH,
        )

    for partner in (pair, cross, diagonal):
        pl.semaphore_signal(barrier, inc=1, device_id=(sp_at, partner), device_id_type=MESH)

    first_loads[0].wait()
    quarter = HEAD_DIM // 4

    def turn(ref, base):
        pieces = []
        for n in range(2):
            cosine, sine = tables[2 * n], tables[2 * n + 1]
            start = base + 2 * n * quarter
            former = ref[start : start + quarter, :].astype(jnp.float32)
            latter = ref[start + quarter : start + 2 * quarter, :].astype(jnp.float32)
            pieces += [former * cosine - latter * sine, former * sine + latter * cosine]
        return pieces

    turned_keys = jnp.concatenate(turn(keys_ref, 0), axis=0)
    near_keys[WINDOW : WINDOW + block_rows, :] = turned_keys.T.astype(near_keys.dtype)
    near_values[:, WINDOW : WINDOW + block_rows] = values_ref[...]
    pl.semaphore_wait(barrier, token_split + 2)

    def halo(n, direction):
        lo = WINDOW if direction == 0 else block_rows
        to = WINDOW + block_rows if direction == 0 else 0
        there = sp_at - 1 if direction == 0 else sp_at + 1
        if n == 0:
            source, target = near_keys.at[lo : lo + WINDOW, :], near_keys.at[to : to + WINDOW, :]
        else:
            source, target = (
                near_values.at[:, lo : lo + WINDOW],
                near_values.at[:, to : to + WINDOW],
            )
        return pltpu.make_async_remote_copy(
            src_ref=source,
            dst_ref=target,
            send_sem=halo_send.at[direction, n],
            recv_sem=halo_recv.at[direction, n],
            device_id=(there, tp_at),
            device_id_type=MESH,
        )

    has_before = sp_at > 0
    has_after = sp_at < token_split - 1

    @pl.when(has_before)
    def _():
        halo(0, 0).start()
        halo(1, 0).start()

    @pl.when(has_after)
    def _():
        halo(0, 1).start()
        halo(1, 1).start()

    for share in shares[:4]:
        share.start()

    for h in range(group):
        for n, piece in enumerate(turn(queries_ref, h * HEAD_DIM)):
            start = h * HEAD_DIM + n * quarter
            turned[start : start + quarter, :] = piece.astype(turned.dtype)

    square = (block_rows, block_rows)
    before = lax.broadcasted_iota(jnp.int32, square, 0)
    after = lax.broadcasted_iota(jnp.int32, square, 1)
    earlier = (before < after) & (before // own == after // own)
    same_place = before == after
    ids_row = [ids_ref[k : k + 1, :] for k in range(TOPK)]
    ids_column = [
        jnp.sum(jnp.where(same_place, row, 0), axis=1, keepdims=True) for row in ids_row
    ]
    half_row = lax.broadcasted_iota(jnp.int32, (1, block_rows), 1) // (2 * own)
    codes, spots = [], []
    for k in range(TOPK):
        found = jnp.zeros(square, jnp.int32)
        for another in range(TOPK):
            found = found + ((ids_column[another] == ids_row[k]) & earlier).astype(jnp.int32)
        rank = jnp.sum(found, axis=0, keepdims=True)
        home = ids_row[k] // experts
        spots.append(home * rows + (ids_row[k] - home * experts) * capacity + rank)
        codes.append(ids_row[k] * rows + half_row * capacity + rank)

    def block_of(row, b):
        return row[:, b * own : (b + 1) * own]

    def column_block(row, b):
        return jnp.where(column == 0, block_of(row, 2 * b), block_of(row, 2 * b + 1))

    column_codes = [
        jnp.concatenate([column_block(code, b) for b in range(halves)], axis=1) for code in codes
    ]
    own_spots = [
        jnp.where(half == 0, column_block(spot, 0), column_block(spot, 1)) for spot in spots
    ]
    slot_at = lax.broadcasted_iota(jnp.int32, (rows, halves * own), 0)

    def chosen(at, expert):
        wanted = slot_at + (at * experts + expert) * rows
        return jnp.where(
            (column_codes[0] == wanted) | (column_codes[1] == wanted), 1.0, 0.0
        ).astype(jnp.bfloat16)

    def remote(stage, i, source, target, where):
        return pltpu.make_async_remote_copy(
            src_ref=source,
            dst_ref=target,
            send_sem=send.at[stage, i],
            recv_sem=recv.at[stage, i],
            device_id=where,
            device_id_type=MESH,
        )

    def partner_of(i):
        return flipped(sp_at, i, token_split)

    near = token_split // 2
    middle = lax.rem(lax.div(sp_at, near) + lax.div(sp_at, max(1, near // 2)), 2)

    def in_order(step):
        last = token_split - 2
        step = jnp.where(step < 2, step, 2 + lax.rem(step + near - 4 + last, last))
        return flipped(step, middle * (near // 2) * lax.div(step, near), token_split)

    def along(i):
        there = partner_of(i)
        return remote(0, i, outgoing.at[there], arrived.at[i, half], (there, tp_at))

    def along_other(i):
        there = partner_of(i)
        return remote(1, i, outgoing_other.at[i], arrived.at[i, other], (there, tp_at))

    def over(i):
        piece = arrived.at[i, half]
        return remote(1, i, piece, piece, (sp_at, cross))

    def cross_back(i):
        return remote(2, i, part.at[i, other], from_cross.at[i], (sp_at, cross))

    def home_copy(i):
        there = partner_of(i)
        return remote(3, i, outgoing.at[there], back.at[sp_at], (there, tp_at))

    shared_over = pltpu.make_async_remote_copy(
        src_ref=shared_part.at[other],
        dst_ref=shared_got,
        send_sem=shared_sem.at[0],
        recv_sem=shared_sem.at[1],
        device_id=(sp_at, cross),
        device_id_type=MESH,
    )

    def weigh_work():
        square = (own, own)
        eye = lax.broadcasted_iota(jnp.int32, square, 0) == lax.broadcasted_iota(
            jnp.int32, square, 1
        )
        slot_of = lax.broadcasted_iota(jnp.int32, (own, token_split * rows), 1)
        weigh = jnp.zeros((own, token_split * rows), jnp.float32)
        for k in range(TOPK):
            spot = jnp.sum(jnp.where(eye, own_spots[k], 0), axis=1, keepdims=True)
            weight = jnp.sum(
                jnp.where(eye, weights_ref[k : k + 1, :], 0.0), axis=1, keepdims=True
            )
            weigh = jnp.where(slot_of == spot, weight, weigh)
        coarse = weigh.astype(jnp.bfloat16)
        weigh_ref[:own, :] = coarse
        weigh_ref[own:, :] = (weigh - coarse.astype(jnp.float32)).astype(jnp.bfloat16)

    weigh_work()

    key_at = lax.broadcasted_iota(jnp.int32, (3 * WINDOW, group * WINDOW), 0)
    query_at = lax.broadcasted_iota(jnp.int32, (3 * WINDOW, group * WINDOW), 1)
    near_enough = jnp.abs(key_at - WINDOW - query_at % WINDOW) <= WINDOW
    head_at = lax.broadcasted_iota(jnp.int32, (1, group * WINDOW), 1) // WINDOW
    sink = jnp.full((1, group * WINDOW), sinks_ref[0])
    for h in range(1, group):
        sink = jnp.where(head_at == h, sinks_ref[h], sink)
    blocks = block_rows // WINDOW
    total_rows = token_split * block_rows

    def attend(block):
        start = block * WINDOW
        query = jnp.concatenate(
            [
                turned[h * HEAD_DIM : (h + 1) * HEAD_DIM, start : start + WINDOW]
                for h in range(group)
            ],
            axis=1,
        )
        allowed = near_enough
        if block == 0:
            allowed = allowed & (key_at + (first_row - WINDOW) >= 0)
        if block == blocks - 1:
            allowed = allowed & (key_at + (first_row + start - WINDOW) < total_rows)
        scores = dot32(near_keys[start : start + 3 * WINDOW, :], query) * HEAD_DIM ** (-0.5)
        scores = jnp.where(allowed, scores, NEG_LARGE)
        highest = jnp.maximum(jnp.max(scores, axis=0, keepdims=True), sink)
        lifted = jnp.exp(scores - highest)
        below = jnp.sum(lifted, axis=0, keepdims=True) + jnp.exp(sink - highest)
        chances = (lifted * (1.0 / below)).astype(jnp.bfloat16)
        result = dot32(near_values[:, start : start + 3 * WINDOW], chances)
        heads = jnp.concatenate(
            [result[:, h * WINDOW : (h + 1) * WINDOW] for h in range(group)], axis=0
        )
        attended[start : start + WINDOW, :] = heads.T.astype(attended.dtype)

    for block in range(1, blocks - 1):
        attend(block)

    @pl.when(has_before)
    def _():
        halo(0, 1).wait_recv()
        halo(1, 1).wait_recv()

    attend(0)

    @pl.when(has_after)
    def _():
        halo(0, 0).wait_recv()
        halo(1, 0).wait_recv()

    if blocks > 1:
        attend(blocks - 1)

    def gather(n, b):
        partner = (cross, diagonal, pair)[n]
        start = pl.multiple_of((2 * b + lax.rem(partner, 2)) * own, own)
        return pltpu.make_async_remote_copy(
            src_ref=attended.at[pl.ds(start, own), :],
            dst_ref=gathered.at[tp_at, b],
            send_sem=gather_send.at[n, b],
            recv_sem=gather_recv.at[n, b],
            device_id=(sp_at, partner),
            device_id_type=MESH,
        )

    for n in range(3):
        for b in range(halves):
            gather(n, b).start()
    for b in range(halves):
        gathered[tp_at, b] = attended[pl.ds(column_start(b), own), :]
    for share in shares[4:]:
        share.start()
    for load in first_loads[1:]:
        load.wait()

    tile = min(width, 512)

    def projected(source, at):
        rows_at = pl.ds(pl.multiple_of(source * group_width, group_width), group_width)
        return dot32(
            gathered[source].reshape(halves * own, group_width), out_weight[rows_at, at]
        )

    @pl.loop(0, width // tile)
    def _(n):
        at = pl.ds(pl.multiple_of(n * tile, tile), tile)
        summed_rows[:, at] = projected(tp_at, at) + residual[:, :, at].reshape(
            halves * own, tile
        ).astype(jnp.float32)

    for n in range(3):
        for b in range(halves):
            gather(n, b).wait_recv()

    squares = jnp.zeros((halves * own, 1), jnp.float32)
    for n in range(width // tile):
        at = slice(n * tile, (n + 1) * tile)
        value = summed_rows[:, at]
        for source in (pair, cross, diagonal):
            value = value + projected(source, at)
        value = value.astype(mixed.dtype)
        mixed[:, :, at] = value.reshape(halves, own, tile)
        value = value.astype(jnp.float32)
        squares = squares + jnp.sum(value * value, axis=1, keepdims=True)
    scale_rows = lax.rsqrt(squares * (1.0 / width) + NORM_EPSILON)
    for n in range(width // tile):
        at = slice(n * tile, (n + 1) * tile)
        value = mixed[:, :, at].reshape(halves * own, tile).astype(jnp.float32)
        column_rows[:, at] = (value * scale_rows * gain_ref[:, at]).astype(column_rows.dtype)

    @pl.loop(1, token_split)
    def _(step):
        i = 1 + lax.rem(step - 1 + middle * (near - 1), token_split - 1)
        there = partner_of(i)
        outgoing[there] = dot32(chosen(there, half), column_rows[...]).astype(outgoing.dtype)
        along(i).start()

        @pl.when(i < near)
        def _():
            outgoing_other[i] = dot32(chosen(there, other), column_rows[...]).astype(
                outgoing_other.dtype
            )
            along_other(i).start()

    for e in range(experts):
        arrived[0, e] = dot32(chosen(sp_at, e), column_rows[...]).astype(arrived.dtype)

    def work(i):
        for e in range(experts):
            x = arrived[i, e]
            for p in range(2):
                hidden[e, :, p * hid : (p + 1) * hid] = silu_times(
                    dot32(x, gate[p, e]), dot32(x, up[p, e])
                ).astype(hidden.dtype)

        @pl.loop(0, width // tile)
        def _(n):
            at = pl.ds(pl.multiple_of(n * tile, tile), tile)
            results = [dot32(hidden[e], down[e, :, at]) for e in range(experts)]
            for b in range(halves):
                if capacity % 8 == 0 and rows == experts * capacity:
                    piece = jnp.concatenate(
                        [result[b * capacity : (b + 1) * capacity] for result in results], axis=0
                    )
                else:
                    piece = jnp.zeros((rows, tile), jnp.float32)
                    into = lax.broadcasted_iota(jnp.int32, (rows, rows), 0)
                    source = lax.broadcasted_iota(jnp.int32, (rows, rows), 1)
                    for e in range(experts):
                        rank = into - e * capacity
                        picked = (
                            (rank >= 0) & (rank < capacity) & (source == rank + b * capacity)
                        )
                        piece = piece + dot32(
                            jnp.where(picked, 1.0, 0.0).astype(jnp.bfloat16),
                            results[e].astype(jnp.bfloat16),
                        )
                part[i, b, :, at] = piece.astype(part.dtype)

    def forward(step):
        i = in_order(step)
        along(i).wait_recv()

        @pl.when(i >= near)
        def _():
            over(i).start()

    for n in range(3):
        loads[n].wait()
        shares[n].wait()
    shared_hidden = silu_times(
        dot32(column_rows[...], shared_gate[...]), dot32(column_rows[...], shared_up[...])
    ).astype(jnp.bfloat16)
    for n in range(width // tile):
        at = slice(n * tile, (n + 1) * tile)
        shared_part[:, :, at] = (
            dot32(shared_hidden, shared_down[:, at])
            .astype(shared_part.dtype)
            .reshape(halves, own, tile)
        )
    for n in range(3, 6):
        loads[n].wait()
        shares[n].wait()

    @pl.loop(0, token_split + 1)
    def _(step):
        @pl.when(step < token_split)
        def _():
            i = in_order(step)

            @pl.when(step >= 1)
            def _():
                over(i).wait_recv()

            work(i)
            cross_back(i).start()

        @pl.when(step == 0)
        def _():
            forward(1)

        @pl.when(step >= 1)
        def _():
            i = in_order(step - 1)
            cross_back(i).wait_recv()
            summed = total(part[i, half], from_cross[i]).astype(back.dtype)

            @pl.when(step == 1)
            def _():
                back[sp_at] = summed

            @pl.when(step >= 2)
            def _():
                along(i).wait_send()
                outgoing[partner_of(i)] = summed
                home_copy(i).start()

        @pl.when(step == 0)
        def _():
            shared_over.start()

        @pl.when(step + 2 < token_split)
        def _():
            forward(step + 2)

    shared_over.wait_recv()

    @pl.loop(1, token_split)
    def _(i):
        home_copy(i).wait_recv()

    for n in range(width // tile):
        at = slice(n * tile, (n + 1) * tile)
        routed = dot32(weigh_ref[...], back[:, :, at].reshape(token_split * rows, tile))
        out_ref[:, at] = (
            total(mixed[half, :, at], shared_part[half, :, at], shared_got[:, at])
            + routed[:own]
            + routed[own:]
        ).astype(out_ref.dtype)

    @pl.loop(0, token_split)
    def _(i):
        cross_back(i).wait_send()

    @pl.loop(1, token_split)
    def _(i):
        over(i).wait_send()
        home_copy(i).wait_send()

    shared_over.wait_send()
    for n in range(3):
        for b in range(halves):
            gather(n, b).wait_send()

    @pl.when(has_before)
    def _():
        halo(0, 0).wait_send()
        halo(1, 0).wait_send()

    @pl.when(has_after)
    def _():
        halo(0, 1).wait_send()
        halo(1, 1).wait_send()


def per_device(
    queries,
    keys,
    values,
    sinks,
    residual,
    out_weight,
    norm_gain,
    shared_gate,
    shared_up,
    shared_down,
    expert_ids,
    route_weights,
    expert_gate,
    expert_up,
    expert_down,
):
    token_split = lax.axis_size("sp")
    width_split = lax.axis_size("tp")
    experts, width, hid = expert_gate.shape
    block_rows, query_width = queries.shape
    if experts != 2 or width_split != 4 or keys.shape[1] != HEAD_DIM:
        raise ValueError("unsupported split")
    own = route_weights.shape[0]
    capacity = max(2, 2 * own * TOPK // (experts * token_split))
    rows = -(-experts * capacity // 16) * 16
    shared_hid = shared_gate.shape[1]
    kind = queries.dtype
    chunk = (rows, width)
    hbm = pl.BlockSpec(memory_space=pltpu.HBM)
    dma = pltpu.SemaphoreType.DMA
    wide_rows = block_rows + 2 * WINDOW
    return pl.pallas_call(
        functools.partial(layer_kernel, token_split, capacity),
        out_shape=jax.ShapeDtypeStruct((own, width), kind),
        in_specs=[pl.BlockSpec(memory_space=pltpu.SMEM)] + [VMEM] * 6 + [hbm] * 9,
        out_specs=VMEM,
        scratch_shapes=[
            pltpu.VMEM((4, HEAD_DIM // 4, block_rows), jnp.float32),
            pltpu.VMEM((2, own, width), kind),
            pltpu.VMEM(out_weight.shape, kind),
            pltpu.VMEM((query_width, block_rows), kind),
            pltpu.VMEM((wide_rows, HEAD_DIM), kind),
            pltpu.VMEM((HEAD_DIM, wide_rows), kind),
            pltpu.VMEM((block_rows, query_width), kind),
            pltpu.VMEM((width_split, 2, own, query_width), kind),
            pltpu.VMEM((2 * own, width), jnp.float32),
            pltpu.VMEM((2, own, width), kind),
            pltpu.VMEM((width, 2 * shared_hid), kind),
            pltpu.VMEM((width, 2 * shared_hid), kind),
            pltpu.VMEM((2 * shared_hid, width), kind),
            pltpu.VMEM((2, experts, width, hid), kind),
            pltpu.VMEM((2, experts, width, hid), kind),
            pltpu.VMEM((experts, 2 * hid, width), kind),
            pltpu.VMEM((2 * own, width), kind),
            pltpu.VMEM((experts, rows, 2 * hid), kind),
            pltpu.VMEM((2 * own, token_split * rows), kind),
            pltpu.VMEM((token_split,) + chunk, kind),
            pltpu.VMEM((token_split // 2,) + chunk, kind),
            pltpu.VMEM((token_split, experts) + chunk, kind),
            pltpu.VMEM((token_split, 2) + chunk, kind),
            pltpu.VMEM((token_split,) + chunk, kind),
            pltpu.VMEM((token_split,) + chunk, kind),
            pltpu.VMEM((2, own, width), kind),
            pltpu.VMEM((own, width), kind),
            dma((6,)),
            dma((6,)),
            dma((6,)),
            dma((4, token_split)),
            dma((4, token_split)),
            dma((2,)),
            dma((4,)),
            dma((2, 2)),
            dma((2, 2)),
            dma((3, 2)),
            dma((3, 2)),
        ],
        compiler_params=pltpu.CompilerParams(
            collective_id=1, has_side_effects=True, vmem_limit_bytes=VMEM_LIMIT
        ),
        name="layer",
    )(
        sinks,
        queries.T,
        keys.T,
        values.T,
        norm_gain.reshape(1, width),
        expert_ids.T,
        route_weights.T,
        jnp.asarray(turn_tables(token_split * block_rows)),
        residual,
        out_weight,
        shared_gate,
        shared_up,
        shared_down,
        expert_gate,
        expert_up,
        expert_down,
    )


def solution(mesh):
    placed = (
        P("sp", "tp"),
        P("sp", "tp"),
        P("sp", "tp"),
        P("tp"),
        P("sp", None),
        P(),
        P(),
        P(None, "tp"),
        P(None, "tp"),
        P("tp", None),
        P("sp", None),
        P(("sp", "tp"), None),
        P("sp", None, "tp"),
        P("sp", None, "tp"),
        P("sp", "tp", None),
    )
    return jax.shard_map(
        per_device, mesh=mesh, in_specs=placed, out_specs=P(("sp", "tp"), None), check_vma=False
    )
```
